32 devices in a mesh: grp: 2 (over y), sp: 4 (over z), tp: 4 (over x, core).
Axes of the slice: x: 2, y: 2, z: 4, core: 2. Of those that a mesh axis runs over, the one named last changes fastest.
Arguments:
- ssm_input: bfloat16 [1024, 1024], P(('grp', 'sp'), 'tp'), parts along dimension 0, may hold values from -6 to 6
- residual_in: bfloat16 [1024, 2048], P(('grp', 'sp')), parts along dimension 0, may hold values from -4 to 4
- log_step: float32 [64], P('tp'), may hold values from -6.91 to -2.3
- decay_real: float32 [64, 64], P('tp'), may hold values from -34 to 0, as said below
- freq: float32 [64, 64], P('tp'), may hold values from 0.5 to 8
- in_real: float32 [64, 64, 16], P('tp'), may hold values from -1 to 1
- in_imag: float32 [64, 64, 16], P('tp'), may hold values from -1 to 1
- out_real: float32 [64, 16, 64], P('tp'), may hold values from -0.5 to 0.5
- out_imag: float32 [64, 16, 64], P('tp'), may hold values from -0.5 to 0.5
- skip: float32 [1024], P('tp'), may hold values from -3 to 3
- w_glu: bfloat16 [1024, 1024], replicated, may hold values from -0.1875 to 0.1875
- b_glu: float32 [1024], replicated, may hold values from -3 to 3
- w_branch: bfloat16 [1024, 2048], replicated, may hold values from -0.1875 to 0.1875
- norm_gain: float32 [2048], replicated, may hold values from 0.1 to 1.9
- w_gate: bfloat16 [2048, 5632], P('sp', 'tp'), may hold values from -0.125 to 0.125
- w_up: bfloat16 [2048, 5632], P('sp', 'tp'), may hold values from -0.125 to 0.125
- w_down: bfloat16 [5632, 2048], P('tp', 'sp'), may hold values from -0.078125 to 0.078125
Outputs:
- mixed: bfloat16 [1024, 2048], P(('grp', 'sp', 'tp')), parts along dimension 0
The draws below stay inside these ranges and needn't reach their ends.
There are 2 independent parts, one for each index of `grp`. The reference program is written for one: setup_inputs(seed, part) draws one part's arguments, and reference() takes and returns one part's arrays. A program takes and returns all parts, laid end to end along the dimension named above; an argument that names none is the same for every part. Nothing has to cross between parts.
Inputs may be any that keep to these rules, and one draw needn't show every extreme that they name: `decay_real`: negative in every entry.
All inputs are finite; a program needn't handle non-finite values.
Results may differ from the reference program's by a relative error of at most 0.015.
Values may be sent and summed in bfloat16 or wider, within the bound.
A program may use at most 128 MiB of HBM per device.

```python
import math
import jax
import jax.numpy as jnp
from jax import lax

D = 2048
FF = 5632
SSM_GROUPS = 64
SSM_GROUP = 16
SSM_STATE = 64
TOK_DEV = 128
SSM_WIDTH = 1024
TOKENS = 512
N_SP = 4


def decay_plan(key):
    subkeys = jax.random.split(jax.random.fold_in(key, 11), 5)
    fast_share = 0.5
    fast_group = jax.random.uniform(subkeys[0], (SSM_GROUPS,), jnp.float32) < fast_share
    slow_rate = jax.random.uniform(subkeys[1], (SSM_GROUPS,), jnp.float32, 0.3, 2.0) / TOKENS
    fast_rate = jax.random.uniform(subkeys[2], (SSM_GROUPS,), jnp.float32, 1.0 / 100.0, 1.0 / 30.0)
    decay_rate = jnp.where(fast_group, fast_rate, slow_rate)
    log_steps = jax.random.uniform(subkeys[3], (SSM_GROUPS,), jnp.float32, math.log(0.001), math.log(0.1))
    spread = jax.random.uniform(subkeys[4], (SSM_GROUPS, SSM_STATE), jnp.float32, 0.5, 1.0)
    return (log_steps, decay_rate, spread)


def draw_log_step(key, part):
    return decay_plan(key)[0]


def draw_decay_real(key, part):
    log_steps, decay_rate, spread = decay_plan(key)
    return -decay_rate[:, None] * spread / jnp.exp(log_steps)[:, None]


def shard_levels(rng, shape, pieces, smallest, largest):
    gain = 1.0
    for position, blocks in pieces:
        heights = jax.random.uniform(jax.random.fold_in(jax.random.fold_in(rng, 6), position), (blocks,), jnp.float32, smallest / len(pieces), largest / len(pieces))
        gain = gain * jnp.repeat(jnp.exp(heights), shape[position] // blocks).reshape((-1,) + (1,) * (len(shape) - 1 - position))
    return gain


def centred(own_key, shape, scale, most, cuts=(), kind=jnp.bfloat16):
    result = scale * jax.random.normal(own_key, shape, jnp.float32)
    if cuts:
        result = result * shard_levels(own_key, shape, cuts, -0.22, 0.18)
    return jnp.clip(result, -most, most).astype(kind)


def setup_inputs(seed: int = 0, part: int = 0) -> dict:
    key_of = jax.random.split(jax.random.key(seed), 18)
    own_keys = jax.random.split(jax.random.fold_in(key_of[17], part), 18)
    return {
        "ssm_input": centred(own_keys[0], (TOKENS, SSM_WIDTH), 1.0, 6.0, ((0, 4), (1, 4))),
        "residual_in": centred(own_keys[1], (TOKENS, D), 0.5, 4.0, ((0, 4),)),
        "log_step": draw_log_step(jax.random.fold_in(key_of[17], 71), part),
        "decay_real": draw_decay_real(jax.random.fold_in(key_of[17], 71), part),
        "freq": jnp.clip(0.5 + 7.5 * jax.random.uniform(key_of[4], (SSM_GROUPS, SSM_STATE), jnp.float32) ** shard_levels(key_of[4], (SSM_GROUPS, SSM_STATE), ((0, 4),), -0.2, 0.2), 0.5, 8.0),
        "in_real": centred(key_of[5], (SSM_GROUPS, SSM_STATE, SSM_GROUP), (2 * SSM_GROUP) ** -0.5, 1.0, ((0, 4),), jnp.float32),
        "in_imag": centred(key_of[6], (SSM_GROUPS, SSM_STATE, SSM_GROUP), (2 * SSM_GROUP) ** -0.5, 1.0, ((0, 4),), jnp.float32),
        "out_real": centred(key_of[7], (SSM_GROUPS, SSM_GROUP, SSM_STATE), (2 * SSM_STATE) ** -0.5, 0.5, ((0, 4),), jnp.float32),
        "out_imag": centred(key_of[8], (SSM_GROUPS, SSM_GROUP, SSM_STATE), (2 * SSM_STATE) ** -0.5, 0.5, ((0, 4),), jnp.float32),
        "skip": centred(key_of[9], (SSM_WIDTH,), 0.5, 3.0, ((0, 4),), jnp.float32),
        "w_glu": centred(key_of[10], (SSM_WIDTH, SSM_WIDTH), SSM_WIDTH ** -0.5, 0.1875),
        "b_glu": centred(key_of[11], (SSM_WIDTH,), 0.5, 3.0, (), jnp.float32),
        "w_branch": centred(key_of[12], (SSM_WIDTH, D), SSM_WIDTH ** -0.5, 0.1875),
        "norm_gain": jnp.clip(1.0 + 0.18 * jax.random.normal(key_of[13], (D,), jnp.float32), 0.1, 1.9),
        "w_gate": centred(key_of[14], (D, FF), D ** -0.5, 0.125, ((0, 4), (1, 4))),
        "w_up": centred(key_of[15], (D, FF), D ** -0.5, 0.125, ((0, 4), (1, 4))),
        "w_down": centred(key_of[16], (FF, D), FF ** -0.5, 0.078125, ((0, 4), (1, 4))),
    }


EPS = 1e-06

def discretize(log_step, decay_real, freq, in_real, in_imag):
    step_size = jnp.exp(log_step)[:, None]
    magnitude = jnp.exp(decay_real * step_size)
    abar_re = magnitude * jnp.cos(freq * step_size)
    abar_im = magnitude * jnp.sin(freq * step_size)
    denominator = decay_real * decay_real + freq * freq
    less_re = abar_re - 1.0
    less_im = abar_im
    hold_re = ((less_re * decay_real + less_im * freq) / denominator)[..., None]
    hold_im = ((less_im * decay_real - less_re * freq) / denominator)[..., None]
    bbar_re = hold_re * in_real - hold_im * in_imag
    bbar_im = hold_re * in_imag + hold_im * in_real
    return (step_size, abar_re, abar_im, bbar_re, bbar_im)

def powers(decay_real, freq, step_size, length):
    steps_up = (jnp.arange(length, dtype=jnp.int32) + 1).astype(jnp.float32)[:, None, None]
    magnitude = jnp.exp((decay_real * step_size)[None] * steps_up)
    phase = (freq * step_size)[None] * steps_up
    return (magnitude * jnp.cos(phase), magnitude * jnp.sin(phase))

def compose(earlier, later):
    a1r, a1i, b1r, b1i = earlier
    a2r, a2i, b2r, b2i = later
    return (a2r * a1r - a2i * a1i, a2r * a1i + a2i * a1r, a2r * b1r - a2i * b1i + b2r, a2r * b1i + a2i * b1r + b2i)

def local_states(inputs, abar_re, abar_im, bbar_re, bbar_im):
    hp = lax.Precision.HIGHEST
    drive_re = jnp.einsum('lgm,gpm->lgp', inputs, bbar_re, precision=hp)
    drive_im = jnp.einsum('lgm,gpm->lgp', inputs, bbar_im, precision=hp)
    full_re = jnp.broadcast_to(abar_re[None], drive_re.shape)
    full_im = jnp.broadcast_to(abar_im[None], drive_re.shape)
    scanned = lax.associative_scan(compose, (full_re, full_im, drive_re, drive_im), axis=0)
    return (scanned[2], scanned[3])

def readout(state_re, state_im, out_real, out_imag, skip_mat, inputs):
    hp = lax.Precision.HIGHEST
    values = jnp.einsum('lgp,gmp->lgm', state_re, out_real, precision=hp) - jnp.einsum('lgp,gmp->lgm', state_im, out_imag, precision=hp) + skip_mat[None] * inputs
    values = jax.nn.gelu(values)
    return values.reshape(values.shape[0], -1).astype(jnp.bfloat16)

def reference(ssm_input, residual_in, log_step, decay_real, freq, in_real, in_imag, out_real, out_imag, skip, w_glu, b_glu, w_branch, norm_gain, w_gate, w_up, w_down):
    step_size, abar_re, abar_im, bbar_re, bbar_im = discretize(log_step, decay_real, freq, in_real, in_imag)
    pow_re, pow_im = powers(decay_real, freq, step_size, TOK_DEV)
    skip_mat = skip.reshape(SSM_GROUPS, SSM_GROUP)
    blocks = ssm_input.astype(jnp.float32).reshape(N_SP, TOK_DEV, SSM_GROUPS, SSM_GROUP)

    def one_block(carried, inputs):
        local_re, local_im = local_states(inputs, abar_re, abar_im, bbar_re, bbar_im)
        state_re = local_re + pow_re * carried[0][None] - pow_im * carried[1][None]
        state_im = local_im + pow_re * carried[1][None] + pow_im * carried[0][None]
        mixer_out = readout(state_re, state_im, out_real, out_imag, skip_mat, inputs)
        return ((state_re[-1], state_im[-1]), mixer_out)
    start_state = (jnp.zeros((SSM_GROUPS, SSM_STATE), jnp.float32), jnp.zeros((SSM_GROUPS, SSM_STATE), jnp.float32))
    unused, outputs = lax.scan(one_block, start_state, blocks)
    mixer_out = outputs.reshape(TOKENS, SSM_WIDTH)
    glu_pre = jnp.dot(mixer_out, w_glu, preferred_element_type=jnp.float32) + b_glu
    gated = (mixer_out.astype(jnp.float32) * jax.nn.sigmoid(glu_pre)).astype(jnp.bfloat16)
    stream = residual_in.astype(jnp.float32) + jnp.dot(gated, w_branch, preferred_element_type=jnp.float32)
    scale_rows = lax.rsqrt(lax.optimization_barrier(jnp.mean(stream * stream, axis=-1, keepdims=True)) + EPS)
    normed = (stream * scale_rows * norm_gain).astype(jnp.bfloat16)
    gate_sum = jnp.dot(normed, w_gate, preferred_element_type=jnp.float32)
    up_sum = jnp.dot(normed, w_up, preferred_element_type=jnp.float32)
    hidden = (jax.nn.silu(gate_sum) * up_sum).astype(jnp.bfloat16)
    return (stream + jnp.dot(hidden, w_down, preferred_element_type=jnp.float32)).astype(jnp.bfloat16)
```

```python
import functools
import math

import jax
import jax.numpy as jnp
from jax import lax
from jax.experimental import pallas as pl
from jax.experimental.pallas import tpu as pltpu
from jax.sharding import PartitionSpec as P

EPS = 1e-06


def prefix(shard, axis, combine, identity):
    count, place = (lax.axis_size(axis), lax.axis_index(axis))
    everything = jax.tree.map(lambda part: lax.all_gather(part, axis), shard)
    start = jax.tree.map(
        lambda part, zero: jnp.broadcast_to(jnp.asarray(zero, part.dtype), part.shape),
        shard,
        identity,
    )

    def lap(k, before):
        reached = k < place
        new = combine(before, jax.tree.map(lambda part: part[k], everything))
        return jax.tree.map(lambda a, b: jnp.where(reached, a, b), new, before)

    return lax.fori_loop(0, count, lap, start)


def discretize(log_step, decay_real, freq, in_real, in_imag):
    step_size = jnp.exp(log_step)[:, None]
    magnitude = jnp.exp(decay_real * step_size)
    abar_re = magnitude * jnp.cos(freq * step_size)
    abar_im = magnitude * jnp.sin(freq * step_size)
    denominator = decay_real * decay_real + freq * freq
    less_re = abar_re - 1.0
    hold_re = ((less_re * decay_real + abar_im * freq) / denominator)[..., None]
    hold_im = ((abar_im * decay_real - less_re * freq) / denominator)[..., None]
    bbar_re = hold_re * in_real - hold_im * in_imag
    bbar_im = hold_re * in_imag + hold_im * in_real
    return (step_size, abar_re, abar_im, bbar_re, bbar_im)


def powers(decay_real, freq, step_size, length):
    steps_up = (jnp.arange(length, dtype=jnp.int32) + 1).astype(jnp.float32)[:, None, None]
    magnitude = jnp.exp((decay_real * step_size)[None] * steps_up)
    phase = (freq * step_size)[None] * steps_up
    return (magnitude * jnp.cos(phase), magnitude * jnp.sin(phase))


def compose(earlier, later):
    a1r, a1i, b1r, b1i = earlier
    a2r, a2i, b2r, b2i = later
    return (
        a2r * a1r - a2i * a1i,
        a2r * a1i + a2i * a1r,
        a2r * b1r - a2i * b1i + b2r,
        a2r * b1i + a2i * b1r + b2i,
    )


def local_states(inputs, decay_real, freq, step_size, bbar_re, bbar_im):
    highest = lax.Precision.HIGHEST
    tok_rows, group_count, unused = inputs.shape
    lanes = group_count * decay_real.shape[1]
    drive_re = jnp.einsum("lgm,gpm->lgp", inputs, bbar_re, precision=highest).reshape(
        tok_rows, lanes
    )
    drive_im = jnp.einsum("lgm,gpm->lgp", inputs, bbar_im, precision=highest).reshape(
        tok_rows, lanes
    )
    span = math.gcd(tok_rows, 16)
    spans = tok_rows // span
    rate = (decay_real * step_size).reshape(lanes)
    turn = (freq * step_size).reshape(lanes)
    later = jnp.arange(span, dtype=jnp.int32)[:, None]
    earlier = jnp.arange(span, dtype=jnp.int32)[None, :]
    lag = (later - earlier).astype(jnp.float32)
    causal = (later >= earlier)[..., None]
    lag_pos = jnp.maximum(lag, 0.0)[..., None]
    table_mag = jnp.exp(rate[None, None] * lag_pos)
    table_re = jnp.where(causal, table_mag * jnp.cos(turn[None, None] * lag_pos), 0.0)
    table_im = jnp.where(causal, table_mag * jnp.sin(turn[None, None] * lag_pos), 0.0)
    block_re = drive_re.reshape(spans, 1, span, lanes)
    block_im = drive_im.reshape(spans, 1, span, lanes)
    inner_re = jnp.sum(table_re[None] * block_re - table_im[None] * block_im, axis=2)
    inner_im = jnp.sum(table_re[None] * block_im + table_im[None] * block_re, axis=2)
    steps_up = (jnp.arange(span, dtype=jnp.int32) + 1).astype(jnp.float32)[:, None]
    pow_mag = jnp.exp(rate[None] * steps_up)
    pow_re = pow_mag * jnp.cos(turn[None] * steps_up)
    pow_im = pow_mag * jnp.sin(turn[None] * steps_up)
    span_re = pow_re[-1]
    span_im = pow_im[-1]

    def carry_step(entering, ends):
        next_re = span_re * entering[0] - span_im * entering[1] + ends[0]
        next_im = span_re * entering[1] + span_im * entering[0] + ends[1]
        return ((next_re, next_im), entering)

    zeros = jnp.zeros((lanes,), jnp.float32)
    unused_carry, entering = lax.scan(
        carry_step, (zeros, zeros), (inner_re[:, -1], inner_im[:, -1])
    )
    state_re = inner_re + pow_re[None] * entering[0][:, None] - pow_im[None] * entering[1][:, None]
    state_im = inner_im + pow_re[None] * entering[1][:, None] + pow_im[None] * entering[0][:, None]
    shape = (tok_rows, group_count, decay_real.shape[1])
    return (state_re.reshape(shape), state_im.reshape(shape))


def readout(state_re, state_im, out_real, out_imag, skip_mat, inputs):
    highest = lax.Precision.HIGHEST
    values = (
        jnp.einsum("lgp,gmp->lgm", state_re, out_real, precision=highest)
        - jnp.einsum("lgp,gmp->lgm", state_im, out_imag, precision=highest)
        + skip_mat[None] * inputs
    )
    values = jax.nn.gelu(values)
    return values.reshape(values.shape[0], -1).astype(jnp.bfloat16)


def row_norm(stream, norm_gain):
    scale_rows = lax.rsqrt(jnp.mean(stream * stream, axis=-1, keepdims=True) + EPS)
    return (stream * scale_rows * norm_gain).astype(jnp.bfloat16)


def gathered_weights(
    ssm_input,
    residual_in,
    log_step,
    decay_real,
    freq,
    in_real,
    in_imag,
    out_real,
    out_imag,
    skip,
    w_glu,
    b_glu,
    w_branch,
    norm_gain,
    w_gate,
    w_up,
    w_down,
):
    tok_rows, width_local = ssm_input.shape
    group_count = log_step.shape[0]
    group_size = in_real.shape[2]
    tp_count = lax.axis_size("tp")
    tp_index = lax.axis_index("tp")
    own_rows = tok_rows // tp_count
    step_size, abar_re, abar_im, bbar_re, bbar_im = discretize(
        log_step, decay_real, freq, in_real, in_imag
    )
    pow_re, pow_im = powers(decay_real, freq, step_size, tok_rows)
    inputs = ssm_input.astype(jnp.float32).reshape(tok_rows, group_count, group_size)
    local_re, local_im = local_states(inputs, decay_real, freq, step_size, bbar_re, bbar_im)
    identity = (
        jnp.ones_like(abar_re),
        jnp.zeros_like(abar_re),
        jnp.zeros_like(abar_re),
        jnp.zeros_like(abar_re),
    )
    carried = prefix((pow_re[-1], pow_im[-1], local_re[-1], local_im[-1]), "sp", compose, identity)
    state_re = local_re + pow_re * carried[2][None] - pow_im * carried[3][None]
    state_im = local_im + pow_re * carried[3][None] + pow_im * carried[2][None]
    mixer_out = readout(
        state_re, state_im, out_real, out_imag, skip.reshape(group_count, group_size), inputs
    )
    mixer_rows = lax.all_to_all(mixer_out, "tp", split_axis=0, concat_axis=1, tiled=True)
    glu_pre = jnp.dot(mixer_rows, w_glu, preferred_element_type=jnp.float32) + b_glu
    gated = (mixer_rows.astype(jnp.float32) * jax.nn.sigmoid(glu_pre)).astype(jnp.bfloat16)
    residual_own = lax.dynamic_slice_in_dim(residual_in, tp_index * own_rows, own_rows, 0)
    stream = residual_own.astype(jnp.float32) + jnp.dot(
        gated, w_branch, preferred_element_type=jnp.float32
    )
    normed = row_norm(stream, norm_gain)
    normed_all = lax.all_gather(normed, "tp", axis=0, tiled=True)
    gate_sum = jnp.dot(
        normed_all,
        lax.all_gather(w_gate, "sp", axis=0, tiled=True),
        preferred_element_type=jnp.float32,
    )
    up_sum = jnp.dot(
        normed_all,
        lax.all_gather(w_up, "sp", axis=0, tiled=True),
        preferred_element_type=jnp.float32,
    )
    hidden = (jax.nn.silu(gate_sum) * up_sum).astype(jnp.bfloat16)
    down_whole = lax.all_gather(w_down, "sp", axis=1, tiled=True)
    summed = lax.psum_scatter(
        jnp.dot(hidden, down_whole, preferred_element_type=jnp.float32).astype(jnp.bfloat16),
        "tp",
        scatter_dimension=0,
        tiled=True,
    ).astype(jnp.float32)
    return (stream + summed).astype(jnp.bfloat16)


MESH = pl.DeviceIdType.MESH
F32 = jnp.float32
BF16 = jnp.bfloat16
NT = (((1,), (1,)), ((), ()))


def greet(n_sp, n_tp, me_s, me_t):
    barrier = pltpu.get_barrier_semaphore()
    for d in range(1, n_sp):
        pl.semaphore_signal(
            barrier, inc=1, device_id={"sp": lax.rem(me_s + d, n_sp)}, device_id_type=MESH
        )
    for d in range(1, n_tp):
        pl.semaphore_signal(
            barrier, inc=1, device_id={"tp": lax.rem(me_t + d, n_tp)}, device_id_type=MESH
        )
    pl.semaphore_wait(barrier, n_sp + n_tp - 2)


def mixer_kernel(
    n_sp, n_tp,
    u_ref, res_ref, ls_ref, dec_ref, frq_ref, inr_ref, ini_ref, outr_ref, outi_ref,
    skip_ref, wglu_ref, bglu_ref, wbr_ref, gain_ref,
    normed_ref, stream_ref,
    wglu, wbr, res, coef, xr, xi, pr_all, pi_all, fin, fin_in, mo, rows_in, glu,
    load_sem, fs, fr, rs, rr,
):
    me_s, me_t = lax.axis_index("sp"), lax.axis_index("tp")
    tok, width = u_ref.shape
    groups, states = dec_ref.shape
    group = width // groups
    lanes = groups * states
    own = tok // n_tp
    loads = [
        pltpu.make_async_copy(
            res_ref.at[pl.ds(pl.multiple_of(me_t * own, own), own)], res, load_sem.at[0]
        ),
        pltpu.make_async_copy(wglu_ref, wglu, load_sem.at[1]),
        pltpu.make_async_copy(wbr_ref, wbr, load_sem.at[2]),
    ]
    for load in loads:
        load.start()

    step = jnp.exp(ls_ref[...])
    dec, frq = dec_ref[...], frq_ref[...]
    mag = jnp.exp(dec * step)
    ar = mag * jnp.cos(frq * step)
    ai = mag * jnp.sin(frq * step)
    den = dec * dec + frq * frq
    less = ar - 1.0
    hr = (less * dec + ai * frq) / den
    hi = (ai * dec - less * frq) / den
    for g in range(groups):
        at = slice(g * states, (g + 1) * states)
        coef[0:1, at] = ar[g : g + 1, :]
        coef[1:2, at] = ai[g : g + 1, :]
        coef[2:3, at] = hr[g : g + 1, :]
        coef[3:4, at] = hi[g : g + 1, :]

    u = u_ref[...]
    spread = (
        lax.broadcasted_iota(jnp.int32, (group, width), 1) % group
        == lax.broadcasted_iota(jnp.int32, (group, width), 0)
    ).astype(BF16)
    part = 128
    row = lax.broadcasted_iota(jnp.int32, (tok, part), 0)
    row8 = lax.broadcasted_iota(jnp.int32, (8, part), 0)
    for c in range(lanes // part):
        at = slice(c * part, (c + 1) * part)
        own_group = (
            (lax.broadcasted_iota(jnp.int32, (part, width), 0) + c * part) // states
            == lax.broadcasted_iota(jnp.int32, (part, width), 1) // group
        )

        def drive(ref):
            wide = jnp.dot(ref[at, :].astype(BF16), spread, preferred_element_type=F32)
            wide = jnp.where(own_group, wide, 0.0).astype(BF16)
            return lax.dot_general(u, wide, NT, preferred_element_type=F32)

        vr, vi = drive(inr_ref), drive(ini_ref)
        cr, ci = coef[2:3, at], coef[3:4, at]
        sr, si = cr * vr - ci * vi, cr * vi + ci * vr
        pr, pi = coef[0:1, at], coef[1:2, at]
        tr, ti = jnp.ones((8, part), F32), jnp.zeros((8, part), F32)
        s = 1
        while s <= tok:
            if s <= 8:
                bit = ((row8 + 1) & s) != 0
                br, bi = jnp.where(bit, pr, 1.0), jnp.where(bit, pi, 0.0)
                tr, ti = tr * br - ti * bi, tr * bi + ti * br
            if s >= 8 and s < tok:
                tr, ti = (
                    jnp.concatenate([tr, tr * pr - ti * pi], 0),
                    jnp.concatenate([ti, tr * pi + ti * pr], 0),
                )
            if s < tok:
                if s < 8:
                    yr = jnp.where(row >= s, pltpu.roll(sr, s, 0), 0.0)
                    yi = jnp.where(row >= s, pltpu.roll(si, s, 0), 0.0)
                else:
                    gap = jnp.zeros((s, part), F32)
                    yr = jnp.concatenate([gap, sr[: tok - s]], 0)
                    yi = jnp.concatenate([gap, si[: tok - s]], 0)
                sr, si = sr + (pr * yr - pi * yi), si + (pr * yi + pi * yr)
            pr, pi = pr * pr - pi * pi, 2.0 * pr * pi
            s *= 2
        xr[:, at], xi[:, at] = sr, si
        pr_all[:, at], pi_all[:, at] = tr, ti
        fin[0:1, at] = sr[tok - 1 : tok]
        fin[1:2, at] = si[tok - 1 : tok]

    greet(n_sp, n_tp, me_s, me_t)
    ends = []
    for d in range(1, n_sp):
        copy = pltpu.make_async_remote_copy(
            src_ref=fin, dst_ref=fin_in.at[d - 1], send_sem=fs.at[d - 1], recv_sem=fr.at[d - 1],
            device_id={"sp": lax.rem(me_s + d, n_sp)}, device_id_type=MESH,
        )
        copy.start()
        ends.append(copy)

    spread = (
        lax.broadcasted_iota(jnp.int32, (states, lanes), 1) % states
        == lax.broadcasted_iota(jnp.int32, (states, lanes), 0)
    ).astype(BF16)
    own_group = (
        lax.broadcasted_iota(jnp.int32, (width, lanes), 0) // group
        == lax.broadcasted_iota(jnp.int32, (width, lanes), 1) // states
    )

    def readout(ref):
        wide = jnp.dot(ref[...].astype(BF16), spread, preferred_element_type=F32)
        return jnp.where(own_group, wide, 0.0).astype(BF16)

    outr, outi = readout(outr_ref), readout(outi_ref)
    for copy in ends:
        copy.wait()
    er, ei = pr_all[tok - 1 : tok, :], pi_all[tok - 1 : tok, :]
    pr, pi = jnp.ones((1, lanes), F32), jnp.zeros((1, lanes), F32)
    cr, ci = jnp.zeros((1, lanes), F32), jnp.zeros((1, lanes), F32)
    for d in range(1, n_sp):
        fr_, fi_ = fin_in[d - 1, 0:1, :], fin_in[d - 1, 1:2, :]
        reached = me_s >= d
        cr = cr + jnp.where(reached, pr * fr_ - pi * fi_, 0.0)
        ci = ci + jnp.where(reached, pr * fi_ + pi * fr_, 0.0)
        pr, pi = pr * er - pi * ei, pr * ei + pi * er
    tr, ti = pr_all[...], pi_all[...]
    sr = (xr[...] + (tr * cr - ti * ci)).astype(BF16)
    si = (xi[...] + (tr * ci + ti * cr)).astype(BF16)
    y = lax.dot_general(sr, outr, NT, preferred_element_type=F32) - lax.dot_general(
        si, outi, NT, preferred_element_type=F32
    )
    y = jax.nn.gelu(y + skip_ref[...] * u.astype(F32))
    mo[...] = y.astype(BF16).reshape(n_tp, own, width)
    turns = []
    for d in range(1, n_tp):
        to = lax.rem(me_t + d, n_tp)
        copy = pltpu.make_async_remote_copy(
            src_ref=mo.at[to], dst_ref=rows_in.at[d - 1], send_sem=rs.at[d - 1],
            recv_sem=rr.at[d - 1], device_id={"tp": to}, device_id_type=MESH,
        )
        copy.start()
        turns.append(copy)
    for load in loads:
        load.wait()

    def source(d):
        return pl.ds(pl.multiple_of(lax.rem(me_t + n_tp - d, n_tp) * width, width), width)

    blocks = [mo[me_t]]
    pre = bglu_ref[...] + jnp.dot(blocks[0], wglu[source(0), :], preferred_element_type=F32)
    for d in range(1, n_tp):
        turns[d - 1].wait()
        blocks.append(rows_in[d - 1])
        pre = pre + jnp.dot(blocks[d], wglu[source(d), :], preferred_element_type=F32)
    glu[...] = pre
    stream = res[...].astype(F32)
    for d in range(n_tp):
        gate = jax.nn.sigmoid(glu[:, source(d)])
        gated = (blocks[d].astype(F32) * gate).astype(BF16)
        stream = stream + jnp.dot(gated, wbr[source(d), :], preferred_element_type=F32)
    stream_ref[...] = stream
    scale = lax.rsqrt(jnp.mean(stream * stream, axis=-1, keepdims=True) + EPS)
    normed_ref[...] = (stream * scale * gain_ref[...]).astype(BF16)


def pieces(total, count):
    tiles = total // 128
    cuts = [128 * (tiles * k // count) for k in range(count)] + [total]
    return [(a, b) for a, b in zip(cuts[:-1], cuts[1:])]


CHUNKS = 3


def ffn_kernel(
    n_sp, n_tp,
    normed_ref, stream_ref, wg_ref, wu_ref, wd_ref,
    out_ref,
    wg, wu, wd, x, part_out, part_in, h, yt_out, yt_in, z_out, z_in,
    load_sem, as_, ar_, bs, br, cs, cr, ds, dr, es, er, gs, gr,
):
    me_s, me_t = lax.axis_index("sp"), lax.axis_index("tp")
    own, width = normed_ref.shape
    depth, hid = wg_ref.shape
    cols = wd_ref.shape[1]
    cuts = pieces(hid, CHUNKS)
    loads = [
        pltpu.make_async_copy(a, b, load_sem.at[k])
        for k, (a, b) in enumerate(((wg_ref, wg), (wu_ref, wu), (wd_ref, wd)))
    ]
    for load in loads:
        load.start()
    greet(n_sp, n_tp, me_s, me_t)

    def send(src, dst, ss, rs, **to):
        copy = pltpu.make_async_remote_copy(
            src_ref=src, dst_ref=dst, send_sem=ss, recv_sem=rs, device_id=to, device_id_type=MESH
        )
        copy.start()
        return copy

    def col(s, size):
        return pl.ds(pl.multiple_of(s * size, size), size)

    turns = []
    for d in range(1, n_sp):
        to = lax.rem(me_s + d, n_sp)
        turns.append(
            send(normed_ref.at[:, col(to, depth)], x.at[d, 0], as_.at[d - 1], ar_.at[d - 1], sp=to)
        )
    x[0, 0] = normed_ref[:, col(me_s, depth)]
    shares = []
    for k in range(n_sp):
        if k:
            turns[k - 1].wait_recv()
        for d in range(1, n_tp):
            src = normed_ref.at[:, col(me_s, depth)] if k == 0 else x.at[k, 0]
            shares.append(
                send(src, x.at[k, d], bs.at[k, d - 1], br.at[k, d - 1],
                     tp=lax.rem(me_t + d, n_tp))
            )
    loads[0].wait()
    loads[1].wait()
    rows = n_tp * own
    far = list(range(1, n_sp))
    parts = {}
    blocks = {}
    for j, (a, b) in enumerate(cuts):
        for k in far:
            if j == 0:
                for d in range(1, n_tp):
                    shares[k * (n_tp - 1) + d - 1].wait_recv()
            block = x[k].reshape(rows, depth)
            part_out[k - 1, 0, :, a:b] = jnp.dot(
                block, wg[:, a:b], preferred_element_type=F32
            ).astype(BF16)
            part_out[k - 1, 1, :, a:b] = jnp.dot(
                block, wu[:, a:b], preferred_element_type=F32
            ).astype(BF16)
            parts[j, k] = send(
                part_out.at[k - 1, :, :, pl.ds(a, b - a)], part_in.at[k - 1, :, :, pl.ds(a, b - a)],
                cs.at[j, k - 1], cr.at[j, k - 1], sp=lax.rem(me_s + n_sp - k, n_sp),
            )
    for d in range(1, n_tp):
        shares[d - 1].wait_recv()
    mine = x[0].reshape(rows, depth)
    spreads = {}
    for j, (a, b) in enumerate(cuts):
        gate = jnp.dot(mine, wg[:, a:b], preferred_element_type=F32)
        up = jnp.dot(mine, wu[:, a:b], preferred_element_type=F32)
        for k in far:
            parts[j, k].wait_recv()
            gate = gate + part_in[k - 1, 0, :, a:b].astype(F32)
            up = up + part_in[k - 1, 1, :, a:b].astype(F32)
        h[0, :, a:b] = (jax.nn.silu(gate) * up).astype(BF16)
        for k in far:
            spreads[j, k] = send(
                h.at[0, :, pl.ds(a, b - a)], h.at[k, :, pl.ds(a, b - a)],
                ds.at[j, k - 1], dr.at[j, k - 1], sp=lax.rem(me_s + k, n_sp),
            )
    loads[2].wait()
    sums = []
    kept = []
    for k in range(n_sp):
        if k:
            for j in range(len(cuts)):
                spreads[j, k].wait_recv()
        y = jnp.dot(h[k], wd[...], preferred_element_type=F32).reshape(n_tp, own, cols)
        kept.append(y[0])
        for d in range(1, n_tp):
            yt_out[k, d - 1] = y[d].astype(BF16)
            sums.append(
                send(yt_out.at[k, d - 1], yt_in.at[k, d - 1], es.at[k, d - 1], er.at[k, d - 1],
                     tp=lax.rem(me_t + n_tp - d, n_tp))
            )
    back = []
    for k in far + [0]:
        z = kept[k]
        for d in range(1, n_tp):
            sums[k * (n_tp - 1) + d - 1].wait_recv()
            z = z + yt_in[k, d - 1].astype(F32)
        if k:
            z_out[k - 1] = z.astype(BF16)
            back.append(
                send(z_out.at[k - 1], z_in.at[k - 1], gs.at[k - 1], gr.at[k - 1],
                     sp=lax.rem(me_s + n_sp - k, n_sp))
            )
        else:
            at = col(me_s, cols)
            out_ref[:, at] = (stream_ref[:, at] + z).astype(BF16)
    for k in far:
        back[k - 1].wait_recv()
        at = col(lax.rem(me_s + k, n_sp), cols)
        out_ref[:, at] = (stream_ref[:, at] + z_in[k - 1].astype(F32)).astype(BF16)
    for copy in turns + shares + list(parts.values()) + list(spreads.values()) + sums + back:
        copy.wait_send()


def moved_rows(
    ssm_input, residual_in, log_step, decay_real, freq, in_real, in_imag, out_real, out_imag,
    skip, w_glu, b_glu, w_branch, norm_gain, w_gate, w_up, w_down,
):
    n_sp, n_tp = lax.axis_size("sp"), lax.axis_size("tp")
    tok, width = ssm_input.shape
    groups, states = decay_real.shape
    group = in_real.shape[2]
    lanes = groups * states
    own = tok // n_tp
    chan, d_model = w_branch.shape
    depth, hid = w_gate.shape
    cols = w_down.shape[1]
    vm = pl.BlockSpec(memory_space=pltpu.VMEM)
    hbm = pl.BlockSpec(memory_space=pl.ANY)
    dma = pltpu.SemaphoreType.DMA
    normed, stream = pl.pallas_call(
        functools.partial(mixer_kernel, n_sp, n_tp),
        out_shape=(
            jax.ShapeDtypeStruct((own, d_model), BF16),
            jax.ShapeDtypeStruct((own, d_model), F32),
        ),
        in_specs=[vm, hbm] + [vm] * 8 + [hbm, vm, hbm, vm],
        out_specs=(vm, vm),
        scratch_shapes=[
            pltpu.VMEM((chan, chan), BF16),
            pltpu.VMEM((chan, d_model), BF16),
            pltpu.VMEM((own, d_model), BF16),
            pltpu.VMEM((8, lanes), F32),
            pltpu.VMEM((tok, lanes), F32),
            pltpu.VMEM((tok, lanes), F32),
            pltpu.VMEM((tok, lanes), F32),
            pltpu.VMEM((tok, lanes), F32),
            pltpu.VMEM((2, lanes), F32),
            pltpu.VMEM((n_sp - 1, 2, lanes), F32),
            pltpu.VMEM((n_tp, own, width), BF16),
            pltpu.VMEM((n_tp - 1, own, width), BF16),
            pltpu.VMEM((own, chan), F32),
            dma((3,)),
            dma((n_sp - 1,)),
            dma((n_sp - 1,)),
            dma((n_tp - 1,)),
            dma((n_tp - 1,)),
        ],
        compiler_params=pltpu.CompilerParams(collective_id=0, has_side_effects=True),
        name="mixer",
    )(
        ssm_input, residual_in, log_step[:, None], decay_real, freq,
        in_real.reshape(lanes, group), in_imag.reshape(lanes, group),
        out_real.reshape(width, states), out_imag.reshape(width, states),
        skip[None], w_glu, b_glu[None], w_branch, norm_gain[None],
    )
    return pl.pallas_call(
        functools.partial(ffn_kernel, n_sp, n_tp),
        out_shape=jax.ShapeDtypeStruct((own, d_model), BF16),
        in_specs=[vm, vm, hbm, hbm, hbm],
        out_specs=vm,
        scratch_shapes=[
            pltpu.VMEM((depth, hid), BF16),
            pltpu.VMEM((depth, hid), BF16),
            pltpu.VMEM((hid, cols), BF16),
            pltpu.VMEM((n_sp, n_tp, own, depth), BF16),
            pltpu.VMEM((n_sp - 1, 2, tok, hid), BF16),
            pltpu.VMEM((n_sp - 1, 2, tok, hid), BF16),
            pltpu.VMEM((n_sp, tok, hid), BF16),
            pltpu.VMEM((n_sp, n_tp - 1, own, cols), BF16),
            pltpu.VMEM((n_sp, n_tp - 1, own, cols), BF16),
            pltpu.VMEM((n_sp - 1, own, cols), BF16),
            pltpu.VMEM((n_sp - 1, own, cols), BF16),
            dma((3,)),
        ]
        + [dma((n_sp - 1,))] * 2
        + [dma((n_sp, n_tp - 1))] * 2
        + [dma((CHUNKS, n_sp - 1))] * 4
        + [dma((n_sp, n_tp - 1))] * 2
        + [dma((n_sp - 1,))] * 2,
        compiler_params=pltpu.CompilerParams(collective_id=1, has_side_effects=True),
        name="feed_forward",
    )(normed, stream, w_gate, w_up, w_down)


def per_device(*arguments):
    tok = arguments[0].shape[0]
    few = lax.axis_size("sp") * tok <= 1024
    return (moved_rows if few else gathered_weights)(*arguments)


def solution(mesh):
    placed = (
        P(("grp", "sp"), "tp"),
        P(("grp", "sp"), None),
        P("tp"),
        P("tp", None),
        P("tp", None),
        P("tp", None, None),
        P("tp", None, None),
        P("tp", None, None),
        P("tp", None, None),
        P("tp"),
        P(),
        P(),
        P(),
        P(),
        P("sp", "tp"),
        P("sp", "tp"),
        P("tp", "sp"),
    )
    return jax.shard_map(
        per_device,
        mesh=mesh,
        in_specs=placed,
        out_specs=P(("grp", "sp", "tp"), None),
        check_vma=False,
    )
```

```python
import functools
import math

import jax
import jax.numpy as jnp
from jax import lax
from jax.experimental import pallas as pl
from jax.experimental.pallas import tpu as pltpu
from jax.sharding import PartitionSpec as P

EPS = 1e-06


def prefix(shard, axis, combine, identity):
    count, place = (lax.axis_size(axis), lax.axis_index(axis))
    everything = jax.tree.map(lambda part: lax.all_gather(part, axis), shard)
    start = jax.tree.map(
        lambda part, zero: jnp.broadcast_to(jnp.asarray(zero, part.dtype), part.shape),
        shard,
        identity,
    )

    def lap(k, before):
        reached = k < place
        new = combine(before, jax.tree.map(lambda part: part[k], everything))
        return jax.tree.map(lambda a, b: jnp.where(reached, a, b), new, before)

    return lax.fori_loop(0, count, lap, start)


def discretize(log_step, decay_real, freq, in_real, in_imag):
    step_size = jnp.exp(log_step)[:, None]
    magnitude = jnp.exp(decay_real * step_size)
    abar_re = magnitude * jnp.cos(freq * step_size)
    abar_im = magnitude * jnp.sin(freq * step_size)
    denominator = decay_real * decay_real + freq * freq
    less_re = abar_re - 1.0
    hold_re = ((less_re * decay_real + abar_im * freq) / denominator)[..., None]
    hold_im = ((abar_im * decay_real - less_re * freq) / denominator)[..., None]
    bbar_re = hold_re * in_real - hold_im * in_imag
    bbar_im = hold_re * in_imag + hold_im * in_real
    return (step_size, abar_re, abar_im, bbar_re, bbar_im)


def powers(decay_real, freq, step_size, length):
    steps_up = (jnp.arange(length, dtype=jnp.int32) + 1).astype(jnp.float32)[:, None, None]
    magnitude = jnp.exp((decay_real * step_size)[None] * steps_up)
    phase = (freq * step_size)[None] * steps_up
    return (magnitude * jnp.cos(phase), magnitude * jnp.sin(phase))


def compose(earlier, later):
    a1r, a1i, b1r, b1i = earlier
    a2r, a2i, b2r, b2i = later
    return (
        a2r * a1r - a2i * a1i,
        a2r * a1i + a2i * a1r,
        a2r * b1r - a2i * b1i + b2r,
        a2r * b1i + a2i * b1r + b2i,
    )


def local_states(inputs, decay_real, freq, step_size, bbar_re, bbar_im):
    highest = lax.Precision.HIGHEST
    tok_rows, group_count, unused = inputs.shape
    lanes = group_count * decay_real.shape[1]
    drive_re = jnp.einsum("lgm,gpm->lgp", inputs, bbar_re, precision=highest).reshape(
        tok_rows, lanes
    )
    drive_im = jnp.einsum("lgm,gpm->lgp", inputs, bbar_im, precision=highest).reshape(
        tok_rows, lanes
    )
    span = math.gcd(tok_rows, 16)
    spans = tok_rows // span
    rate = (decay_real * step_size).reshape(lanes)
    turn = (freq * step_size).reshape(lanes)
    later = jnp.arange(span, dtype=jnp.int32)[:, None]
    earlier = jnp.arange(span, dtype=jnp.int32)[None, :]
    lag = (later - earlier).astype(jnp.float32)
    causal = (later >= earlier)[..., None]
    lag_pos = jnp.maximum(lag, 0.0)[..., None]
    table_mag = jnp.exp(rate[None, None] * lag_pos)
    table_re = jnp.where(causal, table_mag * jnp.cos(turn[None, None] * lag_pos), 0.0)
    table_im = jnp.where(causal, table_mag * jnp.sin(turn[None, None] * lag_pos), 0.0)
    block_re = drive_re.reshape(spans, 1, span, lanes)
    block_im = drive_im.reshape(spans, 1, span, lanes)
    inner_re = jnp.sum(table_re[None] * block_re - table_im[None] * block_im, axis=2)
    inner_im = jnp.sum(table_re[None] * block_im + table_im[None] * block_re, axis=2)
    steps_up = (jnp.arange(span, dtype=jnp.int32) + 1).astype(jnp.float32)[:, None]
    pow_mag = jnp.exp(rate[None] * steps_up)
    pow_re = pow_mag * jnp.cos(turn[None] * steps_up)
    pow_im = pow_mag * jnp.sin(turn[None] * steps_up)
    span_re = pow_re[-1]
    span_im = pow_im[-1]

    def carry_step(entering, ends):
        next_re = span_re * entering[0] - span_im * entering[1] + ends[0]
        next_im = span_re * entering[1] + span_im * entering[0] + ends[1]
        return ((next_re, next_im), entering)

    zeros = jnp.zeros((lanes,), jnp.float32)
    unused_carry, entering = lax.scan(
        carry_step, (zeros, zeros), (inner_re[:, -1], inner_im[:, -1])
    )
    state_re = inner_re + pow_re[None] * entering[0][:, None] - pow_im[None] * entering[1][:, None]
    state_im = inner_im + pow_re[None] * entering[1][:, None] + pow_im[None] * entering[0][:, None]
    shape = (tok_rows, group_count, decay_real.shape[1])
    return (state_re.reshape(shape), state_im.reshape(shape))


def readout(state_re, state_im, out_real, out_imag, skip_mat, inputs):
    highest = lax.Precision.HIGHEST
    values = (
        jnp.einsum("lgp,gmp->lgm", state_re, out_real, precision=highest)
        - jnp.einsum("lgp,gmp->lgm", state_im, out_imag, precision=highest)
        + skip_mat[None] * inputs
    )
    values = jax.nn.gelu(values)
    return values.reshape(values.shape[0], -1).astype(jnp.bfloat16)


def row_norm(stream, norm_gain):
    scale_rows = lax.rsqrt(jnp.mean(stream * stream, axis=-1, keepdims=True) + EPS)
    return (stream * scale_rows * norm_gain).astype(jnp.bfloat16)


def gathered_weights(
    ssm_input,
    residual_in,
    log_step,
    decay_real,
    freq,
    in_real,
    in_imag,
    out_real,
    out_imag,
    skip,
    w_glu,
    b_glu,
    w_branch,
    norm_gain,
    w_gate,
    w_up,
    w_down,
):
    tok_rows, width_local = ssm_input.shape
    group_count = log_step.shape[0]
    group_size = in_real.shape[2]
    tp_count = lax.axis_size("tp")
    tp_index = lax.axis_index("tp")
    own_rows = tok_rows // tp_count
    step_size, abar_re, abar_im, bbar_re, bbar_im = discretize(
        log_step, decay_real, freq, in_real, in_imag
    )
    pow_re, pow_im = powers(decay_real, freq, step_size, tok_rows)
    inputs = ssm_input.astype(jnp.float32).reshape(tok_rows, group_count, group_size)
    local_re, local_im = local_states(inputs, decay_real, freq, step_size, bbar_re, bbar_im)
    identity = (
        jnp.ones_like(abar_re),
        jnp.zeros_like(abar_re),
        jnp.zeros_like(abar_re),
        jnp.zeros_like(abar_re),
    )
    carried = prefix((pow_re[-1], pow_im[-1], local_re[-1], local_im[-1]), "sp", compose, identity)
    state_re = local_re + pow_re * carried[2][None] - pow_im * carried[3][None]
    state_im = local_im + pow_re * carried[3][None] + pow_im * carried[2][None]
    mixer_out = readout(
        state_re, state_im, out_real, out_imag, skip.reshape(group_count, group_size), inputs
    )
    mixer_rows = lax.all_to_all(mixer_out, "tp", split_axis=0, concat_axis=1, tiled=True)
    glu_pre = jnp.dot(mixer_rows, w_glu, preferred_element_type=jnp.float32) + b_glu
    gated = (mixer_rows.astype(jnp.float32) * jax.nn.sigmoid(glu_pre)).astype(jnp.bfloat16)
    residual_own = lax.dynamic_slice_in_dim(residual_in, tp_index * own_rows, own_rows, 0)
    stream = residual_own.astype(jnp.float32) + jnp.dot(
        gated, w_branch, preferred_element_type=jnp.float32
    )
    normed = row_norm(stream, norm_gain)
    normed_all = lax.all_gather(normed, "tp", axis=0, tiled=True)
    gate_sum = jnp.dot(
        normed_all,
        lax.all_gather(w_gate, "sp", axis=0, tiled=True),
        preferred_element_type=jnp.float32,
    )
    up_sum = jnp.dot(
        normed_all,
        lax.all_gather(w_up, "sp", axis=0, tiled=True),
        preferred_element_type=jnp.float32,
    )
    hidden = (jax.nn.silu(gate_sum) * up_sum).astype(jnp.bfloat16)
    down_whole = lax.all_gather(w_down, "sp", axis=1, tiled=True)
    summed = lax.psum_scatter(
        jnp.dot(hidden, down_whole, preferred_element_type=jnp.float32).astype(jnp.bfloat16),
        "tp",
        scatter_dimension=0,
        tiled=True,
    ).astype(jnp.float32)
    return (stream + summed).astype(jnp.bfloat16)


MESH = pl.DeviceIdType.MESH
F32 = jnp.float32
BF16 = jnp.bfloat16
NT = (((1,), (1,)), ((), ()))


def greet(sizes, place):
    barrier = pltpu.get_barrier_semaphore()
    for axis in sizes:
        for d in range(1, sizes[axis]):
            pl.semaphore_signal(
                barrier, inc=1, device_id={axis: lax.rem(place[axis] + d, sizes[axis])},
                device_id_type=MESH,
            )
    pl.semaphore_wait(barrier, sum(sizes.values()) - len(sizes))


def send(src, dst, ss, rs, **to):
    copy = pltpu.make_async_remote_copy(
        src_ref=src, dst_ref=dst, send_sem=ss, recv_sem=rs, device_id=to, device_id_type=MESH
    )
    copy.start()
    return copy


def aligned(index, size):
    return pl.ds(pl.multiple_of(index * size, size), size)


def mixer(
    n_sp, n_tp, during,
    u_ref, res_ref, ls_ref, dec_ref, frq_ref, inr_ref, ini_ref, outr_ref, outi_ref,
    skip_ref, wglu_ref, bglu_ref, wbr_ref, gain_ref,
    normed_ref, stream_ref,
    wglu, wbr, res, coef, xr, xi, pr_all, pi_all, fin, fin_in, mo, rows_in, glu,
    load_sem, fs, fr, rs, rr,
):
    me_s, me_t = lax.axis_index("sp"), lax.axis_index("tp")
    tok, width = u_ref.shape
    groups, states = dec_ref.shape
    group = width // groups
    lanes = groups * states
    own = tok // n_tp
    loads = [
        pltpu.make_async_copy(
            res_ref.at[pl.ds(pl.multiple_of(me_t * own, own), own)], res, load_sem.at[0]
        ),
        pltpu.make_async_copy(wglu_ref, wglu, load_sem.at[1]),
        pltpu.make_async_copy(wbr_ref, wbr, load_sem.at[2]),
    ]
    for load in loads:
        load.start()

    same = lax.broadcasted_iota(jnp.int32, (groups, groups), 0) == lax.broadcasted_iota(
        jnp.int32, (groups, groups), 1
    )
    step = jnp.exp(jnp.sum(jnp.where(same, ls_ref[...], 0.0), axis=1, keepdims=True))
    dec, frq = dec_ref[...], frq_ref[...]
    mag = jnp.exp(dec * step)
    ar = mag * jnp.cos(frq * step)
    ai = mag * jnp.sin(frq * step)
    den = dec * dec + frq * frq
    less = ar - 1.0
    hr = (less * dec + ai * frq) / den
    hi = (ai * dec - less * frq) / den
    for g in range(groups):
        at = slice(g * states, (g + 1) * states)
        coef[0:1, at] = ar[g : g + 1, :]
        coef[1:2, at] = ai[g : g + 1, :]
        coef[2:3, at] = hr[g : g + 1, :]
        coef[3:4, at] = hi[g : g + 1, :]

    u = u_ref[...]
    part = 128
    spread = (
        lax.broadcasted_iota(jnp.int32, (states, part), 1) % states
        == lax.broadcasted_iota(jnp.int32, (states, part), 0)
    ).astype(BF16)
    rows_group = lax.broadcasted_iota(jnp.int32, (width, part), 0) // group
    lane_group = lax.broadcasted_iota(jnp.int32, (width, part), 1) // states

    def spread_out(ref):
        return jnp.dot(ref[...].astype(BF16), spread, preferred_element_type=F32)

    def only(wide, c):
        return jnp.where(rows_group == lane_group + c * (part // states), wide, 0.0).astype(BF16)

    in_r, in_i = spread_out(inr_ref), spread_out(ini_ref)
    row = lax.broadcasted_iota(jnp.int32, (tok, part), 0)
    row8 = lax.broadcasted_iota(jnp.int32, (8, part), 0)
    for c in range(lanes // part):
        at = slice(c * part, (c + 1) * part)
        vr = jnp.dot(u, only(in_r, c), preferred_element_type=F32)
        vi = jnp.dot(u, only(in_i, c), preferred_element_type=F32)
        cr, ci = coef[2:3, at], coef[3:4, at]
        sr, si = cr * vr - ci * vi, cr * vi + ci * vr
        pr, pi = coef[0:1, at], coef[1:2, at]
        tr, ti = jnp.ones((8, part), F32), jnp.zeros((8, part), F32)
        s = 1
        while s <= tok:
            if s <= 8:
                bit = ((row8 + 1) & s) != 0
                br, bi = jnp.where(bit, pr, 1.0), jnp.where(bit, pi, 0.0)
                tr, ti = tr * br - ti * bi, tr * bi + ti * br
            if s >= 8 and s < tok:
                tr, ti = (
                    jnp.concatenate([tr, tr * pr - ti * pi], 0),
                    jnp.concatenate([ti, tr * pi + ti * pr], 0),
                )
            if s < tok:
                if s < 8:
                    yr = jnp.where(row >= s, pltpu.roll(sr, s, 0), 0.0)
                    yi = jnp.where(row >= s, pltpu.roll(si, s, 0), 0.0)
                else:
                    gap = jnp.zeros((s, part), F32)
                    yr = jnp.concatenate([gap, sr[: tok - s]], 0)
                    yi = jnp.concatenate([gap, si[: tok - s]], 0)
                sr, si = sr + (pr * yr - pi * yi), si + (pr * yi + pi * yr)
            pr, pi = pr * pr - pi * pi, 2.0 * pr * pi
            s *= 2
        xr[:, at], xi[:, at] = sr, si
        pr_all[:, at], pi_all[:, at] = tr, ti
        fin[0:1, at] = sr[tok - 1 : tok]
        fin[1:2, at] = si[tok - 1 : tok]

    ends = []
    for d in range(1, n_sp):
        copy = pltpu.make_async_remote_copy(
            src_ref=fin, dst_ref=fin_in.at[d - 1], send_sem=fs.at[d - 1], recv_sem=fr.at[d - 1],
            device_id={"sp": lax.rem(me_s + d, n_sp)}, device_id_type=MESH,
        )
        copy.start()
        ends.append(copy)

    out_r, out_i = spread_out(outr_ref), spread_out(outi_ref)
    outr = jnp.concatenate([only(out_r, c) for c in range(lanes // part)], axis=1)
    outi = jnp.concatenate([only(out_i, c) for c in range(lanes // part)], axis=1)
    for copy in ends:
        copy.wait()
    er, ei = pr_all[tok - 1 : tok, :], pi_all[tok - 1 : tok, :]
    pr, pi = jnp.ones((1, lanes), F32), jnp.zeros((1, lanes), F32)
    cr, ci = jnp.zeros((1, lanes), F32), jnp.zeros((1, lanes), F32)
    for d in range(1, n_sp):
        fr_, fi_ = fin_in[d - 1, 0:1, :], fin_in[d - 1, 1:2, :]
        reached = me_s >= d
        cr = cr + jnp.where(reached, pr * fr_ - pi * fi_, 0.0)
        ci = ci + jnp.where(reached, pr * fi_ + pi * fr_, 0.0)
        pr, pi = pr * er - pi * ei, pr * ei + pi * er
    tr, ti = pr_all[...], pi_all[...]
    sr = (xr[...] + (tr * cr - ti * ci)).astype(BF16)
    si = (xi[...] + (tr * ci + ti * cr)).astype(BF16)
    y = lax.dot_general(sr, outr, NT, preferred_element_type=F32) - lax.dot_general(
        si, outi, NT, preferred_element_type=F32
    )
    y = jax.nn.gelu(y + skip_ref[...] * u.astype(F32))
    mo[...] = y.astype(BF16).reshape(n_tp, own, width)
    turns = []
    for d in range(1, n_tp):
        to = lax.rem(me_t + d, n_tp)
        copy = pltpu.make_async_remote_copy(
            src_ref=mo.at[to], dst_ref=rows_in.at[d - 1], send_sem=rs.at[d - 1],
            recv_sem=rr.at[d - 1], device_id={"tp": to}, device_id_type=MESH,
        )
        copy.start()
        turns.append(copy)
    during()
    for load in loads:
        load.wait()

    def source(d):
        return pl.ds(pl.multiple_of(lax.rem(me_t + n_tp - d, n_tp) * width, width), width)

    blocks = [mo[me_t]]
    pre = bglu_ref[...] + jnp.dot(blocks[0], wglu[source(0), :], preferred_element_type=F32)
    for d in range(1, n_tp):
        turns[d - 1].wait()
        blocks.append(rows_in[d - 1])
        pre = pre + jnp.dot(blocks[d], wglu[source(d), :], preferred_element_type=F32)
    glu[...] = pre
    stream = res[...].astype(F32)
    for d in range(n_tp):
        gate = jax.nn.sigmoid(glu[:, source(d)])
        gated = (blocks[d].astype(F32) * gate).astype(BF16)
        stream = stream + jnp.dot(gated, wbr[source(d), :], preferred_element_type=F32)
    stream_ref[...] = stream
    scale = lax.rsqrt(jnp.mean(stream * stream, axis=-1, keepdims=True) + EPS)
    normed_ref[...] = (stream * scale * gain_ref[...]).astype(BF16)


def pieces(total, count):
    tiles = total // 128
    cuts = [total - 128 * (tiles * k // count) for k in range(count, -1, -1)]
    cuts[0] = 0
    return [(a, b) for a, b in zip(cuts[:-1], cuts[1:])]


CHUNKS = 4
DOWN = 2


def layer_kernel(sizes, *refs):
    n_sp, n_tp = sizes["sp"], sizes["tp"]
    place = {axis: lax.axis_index(axis) for axis in sizes}
    me_g, me_s, me_t = place["grp"], place["sp"], place["tp"]
    wg_ref, wu_ref, wd_ref, out_ref = refs[14:18]
    normed, stream, wgu, wd, x, part_out, part_in, h, y_out, y_in, z_out, z_in = refs[18:30]
    (load_sem, hs, hr, fs, fr, ks, kr, ls, lr, as_, ar_, bs, br, cs, cr, ds, dr, es, er, gs, gr) = (
        refs[30:51]
    )
    mixer_scratch = refs[51:]
    own, d_model = normed.shape
    depth, hid = wg_ref.shape
    cols = wd_ref.shape[1]
    half = me_s // 2
    inner = me_s % 2 != half
    hub = half + 1
    far_hub = 2 - half
    edge = 3 * half
    cuts = pieces(hid, CHUNKS)
    span = depth // 2
    rows_down = hid // 2 // DOWN
    edge_row = (edge % 2) * depth
    edge_col = pl.ds(pl.multiple_of((edge % 2) * cols, cols), cols)

    def edge_rows(g):
        return pl.ds(pl.multiple_of(edge_row + g * span, span), span)

    def down_rows(g, k):
        return pl.ds(pl.multiple_of((g * DOWN + k) * rows_down, rows_down), rows_down)

    def handed(j, start=True):
        a, b = cuts[j]
        copies = []
        for k, ref in enumerate((wg_ref, wu_ref)):
            copies.append(
                pltpu.make_async_remote_copy(
                    src_ref=ref.at[aligned(me_g, span), pl.ds(a, b - a)],
                    dst_ref=wgu.at[k, edge_rows(me_g), pl.ds(a, b - a)],
                    send_sem=hs.at[j, k], recv_sem=hr.at[j, k],
                    device_id={"sp": hub}, device_id_type=MESH,
                )
            )
        return copies

    def handed_down(k):
        return pltpu.make_async_remote_copy(
            src_ref=wd_ref.at[down_rows(me_g, k), :],
            dst_ref=wd.at[down_rows(me_g, k), edge_col],
            send_sem=ks.at[k], recv_sem=kr.at[k], device_id={"sp": hub}, device_id_type=MESH,
        )

    def shared(j):
        a, b = cuts[j]
        piece = wgu.at[:, edge_rows(me_g), pl.ds(a, b - a)]
        return pltpu.make_async_remote_copy(
            src_ref=piece, dst_ref=piece, send_sem=fs.at[j], recv_sem=fr.at[j],
            device_id={"grp": 1 - me_g}, device_id_type=MESH,
        )

    def shared_down(k):
        piece = wd.at[down_rows(me_g, k), edge_col]
        return pltpu.make_async_remote_copy(
            src_ref=piece, dst_ref=piece, send_sem=ls.at[k], recv_sem=lr.at[k],
            device_id={"grp": 1 - me_g}, device_id_type=MESH,
        )

    def hand(j):
        for copy in handed(j):
            copy.start()

    def share(j):
        for copy in handed(j):
            copy.wait_recv()
        shared(j).start()

    own_loads = [
        pltpu.make_async_copy(
            ref, wgu.at[k, aligned(me_s % 2, depth), :], load_sem.at[k]
        )
        for k, ref in enumerate((wg_ref, wu_ref))
    ] + [pltpu.make_async_copy(wd_ref, wd.at[:, aligned(me_s % 2, cols)], load_sem.at[2])]

    greet(sizes, place)

    @pl.when(jnp.logical_not(inner))
    def _():
        hand(0)
        hand(1)

    @pl.when(inner)
    def _():
        for load in own_loads:
            load.start()

    def during():
        @pl.when(jnp.logical_not(inner))
        def _():
            hand(2)

        @pl.when(inner)
        def _():
            share(0)

    mixer(n_sp, n_tp, during, *refs[:14], normed, stream, *mixer_scratch)

    pair = 2 * depth

    def to_hub(q):
        return pltpu.make_async_remote_copy(
            src_ref=normed.at[:, pl.ds(q * pair, pair)], dst_ref=x.at[me_s, 0],
            send_sem=as_.at[q], recv_sem=ar_.at[me_s],
            device_id={"sp": q + 1}, device_id_type=MESH,
        )

    for q in range(2):
        @pl.when(me_s != q + 1)
        def _():
            to_hub(q).start()

    mate = me_t + 1 - 2 * (me_t % 2)
    across = lax.rem(me_t + 2, n_tp)

    def from_hub(s, r, ref, sem):
        return pltpu.make_async_remote_copy(
            src_ref=ref, dst_ref=z_in.at[r], send_sem=gs.at[s], recv_sem=gr.at[r],
            device_id={"sp": s}, device_id_type=MESH,
        )

    @pl.when(jnp.logical_not(inner))
    def _():
        hand(3)
        for j in range(CHUNKS):
            for copy in handed(j):
                copy.wait_send()
        for k in range(DOWN):
            handed_down(k).start()

    @pl.when(inner)
    def _():
        x[me_s, 0] = normed[:, aligned(half, pair)]
        shares = {}
        order = [hub, edge, far_hub, 3 - edge]

        def arrival(s):
            return pltpu.make_async_remote_copy(
                src_ref=x.at[s, 0], dst_ref=x.at[s, 0], send_sem=as_.at[0], recv_sem=ar_.at[s],
                device_id={"sp": far_hub}, device_id_type=MESH,
            )

        def block(s, src, r, slot, to):
            return send(src, x.at[s, slot], bs.at[s, r], br.at[s, r], tp=to)

        for i, s in enumerate(order):
            if i:
                arrival(s).wait_recv()
            src = normed.at[:, aligned(half, pair)] if i == 0 else x.at[s, 0]
            shares[i, 1] = block(s, src, 0, 2, across)
            shares[i, 0] = block(s, src, 1, 1, mate)
        share(1)
        for i, s in enumerate(order):
            shares[i, 1].wait_recv()
            shares[i, 2] = block(s, x.at[s, 2], 2, 3, mate)
        own_loads[0].wait()
        own_loads[1].wait()
        rows = 2 * n_tp * own
        for i, s in enumerate(order):
            shares[i, 0].wait_recv()
            shares[i, 2].wait_recv()
        theirs = x[aligned(1 - half, 2)].reshape(rows, pair)
        parts = []
        for j, (a, b) in enumerate(cuts):
            if j >= 1 and j + 1 < CHUNKS:
                share(j + 1)
            shared(j).wait_recv()
            for k in range(2):
                part_out[k, :, a:b] = jnp.dot(
                    theirs, wgu[k, :, a:b], preferred_element_type=F32
                ).astype(BF16)
            parts.append(
                send(part_out.at[:, :, pl.ds(a, b - a)], part_in.at[:, :, pl.ds(a, b - a)],
                     cs.at[j], cr.at[j], sp=far_hub)
            )
        mine = x[aligned(half, 2)].reshape(rows, pair)
        spreads = []
        for j, (a, b) in enumerate(cuts):
            gate = jnp.dot(mine, wgu[0, :, a:b], preferred_element_type=F32)
            up = jnp.dot(mine, wgu[1, :, a:b], preferred_element_type=F32)
            parts[j].wait_recv()
            gate = gate + part_in[0, :, a:b].astype(F32)
            up = up + part_in[1, :, a:b].astype(F32)
            h[0, :, a:b] = (jax.nn.silu(gate) * up).astype(BF16)
            spreads.append(
                send(h.at[0, :, pl.ds(a, b - a)], h.at[1, :, pl.ds(a, b - a)],
                     ds.at[j], dr.at[j], sp=far_hub)
            )
            if j < DOWN:
                handed_down(j).wait_recv()
                shared_down(j).start()
        own_loads[2].wait()
        for k in range(DOWN):
            shared_down(k).wait_recv()
        slots = [0, 1, 2, 3]
        targets = [me_t, mate, across, 3 - me_t]
        sums = []
        kept = []
        for i in range(2):
            if i:
                for spread in spreads:
                    spread.wait_recv()
            y = jnp.dot(h[i], wd[...], preferred_element_type=F32).reshape(2, n_tp, own, pair)
            kept.append(y[:, 0])
            for r in (2, 3, 1):
                y_out[i, r - 1] = y[:, r].astype(BF16)
                sums.append(
                    send(y_out.at[i, r - 1], y_in.at[i, r - 1], es.at[i, r - 1], er.at[i, r - 1],
                         tp=targets[r])
                )
        backs = []
        for i in (0, 1):
            z = kept[i]
            for n in range(3):
                sums[3 * i + n].wait_recv()
            for r in range(1, n_tp):
                z = z + y_in[i, r - 1].astype(F32)
            z_out[i] = z.astype(BF16)
            if i == 0:
                at = aligned(half, pair)
                spare = me_s % 2
                out_ref[:, at] = (stream[:, at] + z_out[0, spare].astype(F32)).astype(BF16)
                copy = from_hub(edge, half, z_out.at[0, 1 - spare], None)
                copy.start()
                backs.append(copy)
            else:
                for e in range(2):
                    copy = from_hub(2 * (1 - half) + e, half, z_out.at[1, e], None)
                    copy.start()
                    backs.append(copy)
        for copy in list(shares.values()) + parts + spreads + sums + backs:
            copy.wait_send()
        for j in range(CHUNKS):
            shared(j).wait_send()
        for k in range(DOWN):
            shared_down(k).wait_send()

    for q in range(2):
        @pl.when(me_s != q + 1)
        def _():
            pltpu.make_async_remote_copy(
                src_ref=z_in.at[q], dst_ref=z_in.at[q], send_sem=gs.at[0], recv_sem=gr.at[q],
                device_id={"sp": q + 1}, device_id_type=MESH,
            ).wait_recv()
            at = pl.ds(q * pair, pair)
            out_ref[:, at] = (stream[:, at] + z_in[q].astype(F32)).astype(BF16)
            to_hub(q).wait_send()

    @pl.when(jnp.logical_not(inner))
    def _():
        for k in range(DOWN):
            handed_down(k).wait_send()


def moved_rows(
    ssm_input, residual_in, log_step, decay_real, freq, in_real, in_imag, out_real, out_imag,
    skip, w_glu, b_glu, w_branch, norm_gain, w_gate, w_up, w_down,
):
    sizes = {axis: lax.axis_size(axis) for axis in ("grp", "sp", "tp")}
    n_sp, n_tp = sizes["sp"], sizes["tp"]
    tok, width = ssm_input.shape
    groups, states = decay_real.shape
    group = in_real.shape[2]
    lanes = groups * states
    own = tok // n_tp
    chan, d_model = w_branch.shape
    depth, hid = w_gate.shape
    cols = w_down.shape[1]
    pair = 2 * depth
    vm = pl.BlockSpec(memory_space=pltpu.VMEM)
    hbm = pl.BlockSpec(memory_space=pl.ANY)
    dma = pltpu.SemaphoreType.DMA
    vmem = pltpu.VMEM
    return pl.pallas_call(
        functools.partial(layer_kernel, sizes),
        out_shape=jax.ShapeDtypeStruct((own, d_model), BF16),
        in_specs=[vm, hbm] + [vm] * 8 + [hbm, vm, hbm, vm] + [hbm] * 3,
        out_specs=vm,
        scratch_shapes=[
            vmem((own, d_model), BF16),
            vmem((own, d_model), F32),
            vmem((2, pair, hid), BF16),
            vmem((hid, 2 * cols), BF16),
            vmem((n_sp, n_tp, own, pair), BF16),
            vmem((2, 2 * tok, hid), BF16),
            vmem((2, 2 * tok, hid), BF16),
            vmem((2, 2 * tok, hid), BF16),
            vmem((2, n_tp - 1, 2, own, pair), BF16),
            vmem((2, n_tp - 1, 2, own, pair), BF16),
            vmem((2, 2, own, pair), BF16),
            vmem((2, own, pair), BF16),
            dma((3,)),
            dma((CHUNKS, 2)), dma((CHUNKS, 2)),
            dma((CHUNKS,)), dma((CHUNKS,)),
            dma((DOWN,)), dma((DOWN,)), dma((DOWN,)), dma((DOWN,)),
            dma((2,)), dma((n_sp,)),
            dma((n_sp, 3)), dma((n_sp, 3)),
            dma((CHUNKS,)), dma((CHUNKS,)), dma((CHUNKS,)), dma((CHUNKS,)),
            dma((2, n_tp - 1)), dma((2, n_tp - 1)),
            dma((n_sp,)), dma((2,)),
            vmem((chan, chan), BF16),
            vmem((chan, d_model), BF16),
            vmem((own, d_model), BF16),
            vmem((8, lanes), F32),
            vmem((tok, lanes), F32),
            vmem((tok, lanes), F32),
            vmem((tok, lanes), F32),
            vmem((tok, lanes), F32),
            vmem((2, lanes), F32),
            vmem((n_sp - 1, 2, lanes), F32),
            vmem((n_tp, own, width), BF16),
            vmem((n_tp - 1, own, width), BF16),
            vmem((own, chan), F32),
            dma((3,)),
            dma((n_sp - 1,)), dma((n_sp - 1,)),
            dma((n_tp - 1,)), dma((n_tp - 1,)),
        ],
        compiler_params=pltpu.CompilerParams(collective_id=0, has_side_effects=True),
        name="layer",
    )(
        ssm_input, residual_in, log_step[None], decay_real, freq,
        in_real.swapaxes(1, 2).reshape(width, states),
        in_imag.swapaxes(1, 2).reshape(width, states),
        out_real.reshape(width, states), out_imag.reshape(width, states),
        skip[None], w_glu, b_glu[None], w_branch, norm_gain[None], w_gate, w_up, w_down,
    )


def per_device(*arguments):
    sizes = tuple(lax.axis_size(axis) for axis in ("grp", "sp", "tp"))
    return (moved_rows if sizes == (2, 4, 4) else gathered_weights)(*arguments)


def solution(mesh):
    placed = (
        P(("grp", "sp"), "tp"),
        P(("grp", "sp"), None),
        P("tp"),
        P("tp", None),
        P("tp", None),
        P("tp", None, None),
        P("tp", None, None),
        P("tp", None, None),
        P("tp", None, None),
        P("tp"),
        P(),
        P(),
        P(),
        P(),
        P("sp", "tp"),
        P("sp", "tp"),
        P("tp", "sp"),
    )
    return jax.shard_map(
        per_device,
        mesh=mesh,
        in_specs=placed,
        out_specs=P(("grp", "sp", "tp"), None),
        check_vma=False,
    )
```

```python
import functools
import math

import jax
import jax.numpy as jnp
from jax import lax
from jax.experimental import pallas as pl
from jax.experimental.pallas import tpu as pltpu
from jax.sharding import PartitionSpec as P

EPS = 1e-06


def prefix(shard, axis, combine, identity):
    count, place = (lax.axis_size(axis), lax.axis_index(axis))
    everything = jax.tree.map(lambda part: lax.all_gather(part, axis), shard)
    start = jax.tree.map(
        lambda part, zero: jnp.broadcast_to(jnp.asarray(zero, part.dtype), part.shape),
        shard,
        identity,
    )

    def lap(k, before):
        reached = k < place
        new = combine(before, jax.tree.map(lambda part: part[k], everything))
        return jax.tree.map(lambda a, b: jnp.where(reached, a, b), new, before)

    return lax.fori_loop(0, count, lap, start)


def discretize(log_step, decay_real, freq, in_real, in_imag):
    step_size = jnp.exp(log_step)[:, None]
    magnitude = jnp.exp(decay_real * step_size)
    abar_re = magnitude * jnp.cos(freq * step_size)
    abar_im = magnitude * jnp.sin(freq * step_size)
    denominator = decay_real * decay_real + freq * freq
    less_re = abar_re - 1.0
    hold_re = ((less_re * decay_real + abar_im * freq) / denominator)[..., None]
    hold_im = ((abar_im * decay_real - less_re * freq) / denominator)[..., None]
    bbar_re = hold_re * in_real - hold_im * in_imag
    bbar_im = hold_re * in_imag + hold_im * in_real
    return (step_size, abar_re, abar_im, bbar_re, bbar_im)


def powers(decay_real, freq, step_size, length):
    steps_up = (jnp.arange(length, dtype=jnp.int32) + 1).astype(jnp.float32)[:, None, None]
    magnitude = jnp.exp((decay_real * step_size)[None] * steps_up)
    phase = (freq * step_size)[None] * steps_up
    return (magnitude * jnp.cos(phase), magnitude * jnp.sin(phase))


def compose(earlier, later):
    a1r, a1i, b1r, b1i = earlier
    a2r, a2i, b2r, b2i = later
    return (
        a2r * a1r - a2i * a1i,
        a2r * a1i + a2i * a1r,
        a2r * b1r - a2i * b1i + b2r,
        a2r * b1i + a2i * b1r + b2i,
    )


def local_states(inputs, decay_real, freq, step_size, bbar_re, bbar_im):
    highest = lax.Precision.HIGHEST
    tok_rows, group_count, unused = inputs.shape
    lanes = group_count * decay_real.shape[1]
    drive_re = jnp.einsum("lgm,gpm->lgp", inputs, bbar_re, precision=highest).reshape(
        tok_rows, lanes
    )
    drive_im = jnp.einsum("lgm,gpm->lgp", inputs, bbar_im, precision=highest).reshape(
        tok_rows, lanes
    )
    span = math.gcd(tok_rows, 16)
    spans = tok_rows // span
    rate = (decay_real * step_size).reshape(lanes)
    turn = (freq * step_size).reshape(lanes)
    later = jnp.arange(span, dtype=jnp.int32)[:, None]
    earlier = jnp.arange(span, dtype=jnp.int32)[None, :]
    lag = (later - earlier).astype(jnp.float32)
    causal = (later >= earlier)[..., None]
    lag_pos = jnp.maximum(lag, 0.0)[..., None]
    table_mag = jnp.exp(rate[None, None] * lag_pos)
    table_re = jnp.where(causal, table_mag * jnp.cos(turn[None, None] * lag_pos), 0.0)
    table_im = jnp.where(causal, table_mag * jnp.sin(turn[None, None] * lag_pos), 0.0)
    block_re = drive_re.reshape(spans, 1, span, lanes)
    block_im = drive_im.reshape(spans, 1, span, lanes)
    inner_re = jnp.sum(table_re[None] * block_re - table_im[None] * block_im, axis=2)
    inner_im = jnp.sum(table_re[None] * block_im + table_im[None] * block_re, axis=2)
    steps_up = (jnp.arange(span, dtype=jnp.int32) + 1).astype(jnp.float32)[:, None]
    pow_mag = jnp.exp(rate[None] * steps_up)
    pow_re = pow_mag * jnp.cos(turn[None] * steps_up)
    pow_im = pow_mag * jnp.sin(turn[None] * steps_up)
    span_re = pow_re[-1]
    span_im = pow_im[-1]

    def carry_step(entering, ends):
        next_re = span_re * entering[0] - span_im * entering[1] + ends[0]
        next_im = span_re * entering[1] + span_im * entering[0] + ends[1]
        return ((next_re, next_im), entering)

    zeros = jnp.zeros((lanes,), jnp.float32)
    unused_carry, entering = lax.scan(
        carry_step, (zeros, zeros), (inner_re[:, -1], inner_im[:, -1])
    )
    state_re = inner_re + pow_re[None] * entering[0][:, None] - pow_im[None] * entering[1][:, None]
    state_im = inner_im + pow_re[None] * entering[1][:, None] + pow_im[None] * entering[0][:, None]
    shape = (tok_rows, group_count, decay_real.shape[1])
    return (state_re.reshape(shape), state_im.reshape(shape))


def readout(state_re, state_im, out_real, out_imag, skip_mat, inputs):
    highest = lax.Precision.HIGHEST
    values = (
        jnp.einsum("lgp,gmp->lgm", state_re, out_real, precision=highest)
        - jnp.einsum("lgp,gmp->lgm", state_im, out_imag, precision=highest)
        + skip_mat[None] * inputs
    )
    values = jax.nn.gelu(values)
    return values.reshape(values.shape[0], -1).astype(jnp.bfloat16)


def row_norm(stream, norm_gain):
    scale_rows = lax.rsqrt(jnp.mean(stream * stream, axis=-1, keepdims=True) + EPS)
    return (stream * scale_rows * norm_gain).astype(jnp.bfloat16)


def gathered_weights(
    ssm_input,
    residual_in,
    log_step,
    decay_real,
    freq,
    in_real,
    in_imag,
    out_real,
    out_imag,
    skip,
    w_glu,
    b_glu,
    w_branch,
    norm_gain,
    w_gate,
    w_up,
    w_down,
):
    tok_rows, width_local = ssm_input.shape
    group_count = log_step.shape[0]
    group_size = in_real.shape[2]
    tp_count = lax.axis_size("tp")
    tp_index = lax.axis_index("tp")
    own_rows = tok_rows // tp_count
    step_size, abar_re, abar_im, bbar_re, bbar_im = discretize(
        log_step, decay_real, freq, in_real, in_imag
    )
    pow_re, pow_im = powers(decay_real, freq, step_size, tok_rows)
    inputs = ssm_input.astype(jnp.float32).reshape(tok_rows, group_count, group_size)
    local_re, local_im = local_states(inputs, decay_real, freq, step_size, bbar_re, bbar_im)
    identity = (
        jnp.ones_like(abar_re),
        jnp.zeros_like(abar_re),
        jnp.zeros_like(abar_re),
        jnp.zeros_like(abar_re),
    )
    carried = prefix((pow_re[-1], pow_im[-1], local_re[-1], local_im[-1]), "sp", compose, identity)
    state_re = local_re + pow_re * carried[2][None] - pow_im * carried[3][None]
    state_im = local_im + pow_re * carried[3][None] + pow_im * carried[2][None]
    mixer_out = readout(
        state_re, state_im, out_real, out_imag, skip.reshape(group_count, group_size), inputs
    )
    mixer_rows = lax.all_to_all(mixer_out, "tp", split_axis=0, concat_axis=1, tiled=True)
    glu_pre = jnp.dot(mixer_rows, w_glu, preferred_element_type=jnp.float32) + b_glu
    gated = (mixer_rows.astype(jnp.float32) * jax.nn.sigmoid(glu_pre)).astype(jnp.bfloat16)
    residual_own = lax.dynamic_slice_in_dim(residual_in, tp_index * own_rows, own_rows, 0)
    stream = residual_own.astype(jnp.float32) + jnp.dot(
        gated, w_branch, preferred_element_type=jnp.float32
    )
    normed = row_norm(stream, norm_gain)
    normed_all = lax.all_gather(normed, "tp", axis=0, tiled=True)
    gate_sum = jnp.dot(
        normed_all,
        lax.all_gather(w_gate, "sp", axis=0, tiled=True),
        preferred_element_type=jnp.float32,
    )
    up_sum = jnp.dot(
        normed_all,
        lax.all_gather(w_up, "sp", axis=0, tiled=True),
        preferred_element_type=jnp.float32,
    )
    hidden = (jax.nn.silu(gate_sum) * up_sum).astype(jnp.bfloat16)
    down_whole = lax.all_gather(w_down, "sp", axis=1, tiled=True)
    summed = lax.psum_scatter(
        jnp.dot(hidden, down_whole, preferred_element_type=jnp.float32).astype(jnp.bfloat16),
        "tp",
        scatter_dimension=0,
        tiled=True,
    ).astype(jnp.float32)
    return (stream + summed).astype(jnp.bfloat16)


MESH = pl.DeviceIdType.MESH
F32 = jnp.float32
BF16 = jnp.bfloat16
NT = (((1,), (1,)), ((), ()))


def greet(sizes, place):
    barrier = pltpu.get_barrier_semaphore()
    for axis in sizes:
        for d in range(1, sizes[axis]):
            pl.semaphore_signal(
                barrier, inc=1, device_id={axis: lax.rem(place[axis] + d, sizes[axis])},
                device_id_type=MESH,
            )
    pl.semaphore_wait(barrier, sum(sizes.values()) - len(sizes))


def send(src, dst, ss, rs, **to):
    copy = pltpu.make_async_remote_copy(
        src_ref=src, dst_ref=dst, send_sem=ss, recv_sem=rs, device_id=to, device_id_type=MESH
    )
    copy.start()
    return copy


def aligned(index, size):
    return pl.ds(pl.multiple_of(index * size, size), size)


def mixer(
    n_sp, n_tp, during,
    u_ref, res_ref, ls_ref, dec_ref, frq_ref, inr_ref, ini_ref, outr_ref, outi_ref,
    skip_ref, wglu_ref, bglu_ref, wbr_ref, gain_ref,
    normed_ref, stream_ref,
    wglu, wbr, res, coef, xr, xi, pr_all, pi_all, fin, fin_in, mo, rows_in, glu,
    load_sem, fs, fr, rs, rr,
):
    me_s, me_t = lax.axis_index("sp"), lax.axis_index("tp")
    tok, width = u_ref.shape
    groups, states = dec_ref.shape
    group = width // groups
    lanes = groups * states
    own = tok // n_tp
    loads = [
        pltpu.make_async_copy(
            res_ref.at[pl.ds(pl.multiple_of(me_t * own, own), own)], res, load_sem.at[0]
        ),
        pltpu.make_async_copy(wglu_ref, wglu, load_sem.at[1]),
        pltpu.make_async_copy(wbr_ref, wbr, load_sem.at[2]),
    ]
    for load in loads:
        load.start()

    same = lax.broadcasted_iota(jnp.int32, (groups, groups), 0) == lax.broadcasted_iota(
        jnp.int32, (groups, groups), 1
    )
    step = jnp.exp(jnp.sum(jnp.where(same, ls_ref[...], 0.0), axis=1, keepdims=True))
    dec, frq = dec_ref[...], frq_ref[...]
    mag = jnp.exp(dec * step)
    ar = mag * jnp.cos(frq * step)
    ai = mag * jnp.sin(frq * step)
    den = dec * dec + frq * frq
    less = ar - 1.0
    hr = (less * dec + ai * frq) / den
    hi = (ai * dec - less * frq) / den
    for g in range(groups):
        at = slice(g * states, (g + 1) * states)
        coef[0:1, at] = ar[g : g + 1, :]
        coef[1:2, at] = ai[g : g + 1, :]
        coef[2:3, at] = hr[g : g + 1, :]
        coef[3:4, at] = hi[g : g + 1, :]

    u = u_ref[...]
    part = 128
    spread = (
        lax.broadcasted_iota(jnp.int32, (states, part), 1) % states
        == lax.broadcasted_iota(jnp.int32, (states, part), 0)
    ).astype(BF16)
    rows_group = lax.broadcasted_iota(jnp.int32, (width, part), 0) // group
    lane_group = lax.broadcasted_iota(jnp.int32, (width, part), 1) // states

    def spread_out(ref):
        return jnp.dot(ref[...].astype(BF16), spread, preferred_element_type=F32)

    def only(wide, c):
        return jnp.where(rows_group == lane_group + c * (part // states), wide, 0.0).astype(BF16)

    in_r, in_i = spread_out(inr_ref), spread_out(ini_ref)
    row = lax.broadcasted_iota(jnp.int32, (tok, part), 0)
    row8 = lax.broadcasted_iota(jnp.int32, (8, part), 0)
    for c in range(lanes // part):
        at = slice(c * part, (c + 1) * part)
        vr = jnp.dot(u, only(in_r, c), preferred_element_type=F32)
        vi = jnp.dot(u, only(in_i, c), preferred_element_type=F32)
        cr, ci = coef[2:3, at], coef[3:4, at]
        sr, si = cr * vr - ci * vi, cr * vi + ci * vr
        pr, pi = coef[0:1, at], coef[1:2, at]
        tr, ti = jnp.ones((8, part), F32), jnp.zeros((8, part), F32)
        s = 1
        while s <= tok:
            if s <= 8:
                bit = ((row8 + 1) & s) != 0
                br, bi = jnp.where(bit, pr, 1.0), jnp.where(bit, pi, 0.0)
                tr, ti = tr * br - ti * bi, tr * bi + ti * br
            if s >= 8 and s < tok:
                tr, ti = (
                    jnp.concatenate([tr, tr * pr - ti * pi], 0),
                    jnp.concatenate([ti, tr * pi + ti * pr], 0),
                )
            if s < tok:
                if s < 8:
                    yr = jnp.where(row >= s, pltpu.roll(sr, s, 0), 0.0)
                    yi = jnp.where(row >= s, pltpu.roll(si, s, 0), 0.0)
                else:
                    gap = jnp.zeros((s, part), F32)
                    yr = jnp.concatenate([gap, sr[: tok - s]], 0)
                    yi = jnp.concatenate([gap, si[: tok - s]], 0)
                sr, si = sr + (pr * yr - pi * yi), si + (pr * yi + pi * yr)
            pr, pi = pr * pr - pi * pi, 2.0 * pr * pi
            s *= 2
        xr[:, at], xi[:, at] = sr, si
        pr_all[:, at], pi_all[:, at] = tr, ti
        fin[0:1, at] = sr[tok - 1 : tok]
        fin[1:2, at] = si[tok - 1 : tok]

    ends = []
    for d in range(1, n_sp):
        copy = pltpu.make_async_remote_copy(
            src_ref=fin, dst_ref=fin_in.at[d - 1], send_sem=fs.at[d - 1], recv_sem=fr.at[d - 1],
            device_id={"sp": lax.rem(me_s + d, n_sp)}, device_id_type=MESH,
        )
        copy.start()
        ends.append(copy)

    out_r, out_i = spread_out(outr_ref), spread_out(outi_ref)
    outr = jnp.concatenate([only(out_r, c) for c in range(lanes // part)], axis=1)
    outi = jnp.concatenate([only(out_i, c) for c in range(lanes // part)], axis=1)
    for copy in ends:
        copy.wait()
    er, ei = pr_all[tok - 1 : tok, :], pi_all[tok - 1 : tok, :]
    pr, pi = jnp.ones((1, lanes), F32), jnp.zeros((1, lanes), F32)
    cr, ci = jnp.zeros((1, lanes), F32), jnp.zeros((1, lanes), F32)
    for d in range(1, n_sp):
        fr_, fi_ = fin_in[d - 1, 0:1, :], fin_in[d - 1, 1:2, :]
        reached = me_s >= d
        cr = cr + jnp.where(reached, pr * fr_ - pi * fi_, 0.0)
        ci = ci + jnp.where(reached, pr * fi_ + pi * fr_, 0.0)
        pr, pi = pr * er - pi * ei, pr * ei + pi * er
    tr, ti = pr_all[...], pi_all[...]
    sr = (xr[...] + (tr * cr - ti * ci)).astype(BF16)
    si = (xi[...] + (tr * ci + ti * cr)).astype(BF16)
    y = lax.dot_general(sr, outr, NT, preferred_element_type=F32) - lax.dot_general(
        si, outi, NT, preferred_element_type=F32
    )
    y = jax.nn.gelu(y + skip_ref[...] * u.astype(F32))
    mo[...] = y.astype(BF16).reshape(n_tp, own, width)
    turns = []
    for d in range(1, n_tp):
        to = lax.rem(me_t + d, n_tp)
        copy = pltpu.make_async_remote_copy(
            src_ref=mo.at[to], dst_ref=rows_in.at[d - 1], send_sem=rs.at[d - 1],
            recv_sem=rr.at[d - 1], device_id={"tp": to}, device_id_type=MESH,
        )
        copy.start()
        turns.append(copy)
    during()
    for load in loads:
        load.wait()

    def source(d):
        return pl.ds(pl.multiple_of(lax.rem(me_t + n_tp - d, n_tp) * width, width), width)

    blocks = [mo[me_t]]
    pre = bglu_ref[...] + jnp.dot(blocks[0], wglu[source(0), :], preferred_element_type=F32)
    for d in range(1, n_tp):
        turns[d - 1].wait()
        blocks.append(rows_in[d - 1])
        pre = pre + jnp.dot(blocks[d], wglu[source(d), :], preferred_element_type=F32)
    glu[...] = pre
    stream = res[...].astype(F32)
    for d in range(n_tp):
        gate = jax.nn.sigmoid(glu[:, source(d)])
        gated = (blocks[d].astype(F32) * gate).astype(BF16)
        stream = stream + jnp.dot(gated, wbr[source(d), :], preferred_element_type=F32)
    stream_ref[...] = stream
    scale = lax.rsqrt(jnp.mean(stream * stream, axis=-1, keepdims=True) + EPS)
    normed_ref[...] = (stream * scale * gain_ref[...]).astype(BF16)


def pieces(total, count):
    tiles = total // 128
    cuts = [total - 128 * (tiles * k // count) for k in range(count, -1, -1)]
    cuts[0] = 0
    return [(a, b) for a, b in zip(cuts[:-1], cuts[1:])]


CHUNKS = 4
DOWN = 2


def layer_kernel(sizes, *refs):
    n_sp, n_tp = sizes["sp"], sizes["tp"]
    place = {axis: lax.axis_index(axis) for axis in sizes}
    me_g, me_s, me_t = place["grp"], place["sp"], place["tp"]
    wg_ref, wu_ref, wd_ref, out_ref = refs[14:18]
    normed, stream, wgu, wd, x, part_out, part_in, h, y_out, y_in, z_out, z_in = refs[18:30]
    (load_sem, hs, hr, fs, fr, ks, kr, ls, lr, as_, ar_, bs, br, cs, cr, ds, dr, es, er, gs, gr) = (
        refs[30:51]
    )
    mixer_scratch = refs[51:]
    own, d_model = normed.shape
    depth, hid = wg_ref.shape
    cols = wd_ref.shape[1]
    half = me_s // 2
    inner = me_s % 2 != half
    hub = half + 1
    far_hub = 2 - half
    edge = 3 * half
    cuts = pieces(hid, CHUNKS)
    span = depth // 2
    rows_down = hid // 2 // DOWN
    edge_row = (edge % 2) * depth
    edge_col = pl.ds(pl.multiple_of((edge % 2) * cols, cols), cols)

    def edge_rows(g):
        return pl.ds(pl.multiple_of(edge_row + g * span, span), span)

    def down_rows(g, k):
        return pl.ds(pl.multiple_of((g * DOWN + k) * rows_down, rows_down), rows_down)

    def handed(j, start=True):
        a, b = cuts[j]
        copies = []
        for k, ref in enumerate((wg_ref, wu_ref)):
            copies.append(
                pltpu.make_async_remote_copy(
                    src_ref=ref.at[aligned(me_g, span), pl.ds(a, b - a)],
                    dst_ref=wgu.at[k, edge_rows(me_g), pl.ds(a, b - a)],
                    send_sem=hs.at[j, k], recv_sem=hr.at[j, k],
                    device_id={"sp": hub}, device_id_type=MESH,
                )
            )
        return copies

    def handed_down(k):
        return pltpu.make_async_remote_copy(
            src_ref=wd_ref.at[down_rows(me_g, k), :],
            dst_ref=wd.at[down_rows(me_g, k), edge_col],
            send_sem=ks.at[k], recv_sem=kr.at[k], device_id={"sp": hub}, device_id_type=MESH,
        )

    def shared(j):
        a, b = cuts[j]
        piece = wgu.at[:, edge_rows(me_g), pl.ds(a, b - a)]
        return pltpu.make_async_remote_copy(
            src_ref=piece, dst_ref=piece, send_sem=fs.at[j], recv_sem=fr.at[j],
            device_id={"grp": 1 - me_g}, device_id_type=MESH,
        )

    def shared_down(k):
        piece = wd.at[down_rows(me_g, k), edge_col]
        return pltpu.make_async_remote_copy(
            src_ref=piece, dst_ref=piece, send_sem=ls.at[k], recv_sem=lr.at[k],
            device_id={"grp": 1 - me_g}, device_id_type=MESH,
        )

    def hand(j):
        for copy in handed(j):
            copy.start()

    def share(j):
        for copy in handed(j):
            copy.wait_recv()
        shared(j).start()

    own_loads = [
        pltpu.make_async_copy(
            ref, wgu.at[k, aligned(me_s % 2, depth), :], load_sem.at[k]
        )
        for k, ref in enumerate((wg_ref, wu_ref))
    ] + [pltpu.make_async_copy(wd_ref, wd.at[:, aligned(me_s % 2, cols)], load_sem.at[2])]

    greet(sizes, place)

    @pl.when(jnp.logical_not(inner))
    def _():
        hand(0)
        hand(1)

    @pl.when(inner)
    def _():
        for load in own_loads:
            load.start()

    def during():
        @pl.when(jnp.logical_not(inner))
        def _():
            hand(2)

        @pl.when(inner)
        def _():
            share(0)

    mixer(n_sp, n_tp, during, *refs[:14], normed, stream, *mixer_scratch)

    pair = 2 * depth

    def to_hub(q):
        return pltpu.make_async_remote_copy(
            src_ref=normed.at[:, pl.ds(q * pair, pair)], dst_ref=x.at[me_s, 0],
            send_sem=as_.at[q], recv_sem=ar_.at[me_s],
            device_id={"sp": q + 1}, device_id_type=MESH,
        )

    for q in range(2):
        @pl.when(me_s != q + 1)
        def _():
            to_hub(q).start()

    mate = me_t + 1 - 2 * (me_t % 2)
    across = lax.rem(me_t + 2, n_tp)

    def from_hub(s, r, ref, sem):
        return pltpu.make_async_remote_copy(
            src_ref=ref, dst_ref=z_in.at[r], send_sem=gs.at[s], recv_sem=gr.at[r],
            device_id={"sp": s}, device_id_type=MESH,
        )

    @pl.when(jnp.logical_not(inner))
    def _():
        hand(3)
        for j in range(CHUNKS):
            for copy in handed(j):
                copy.wait_send()
        for k in range(DOWN):
            handed_down(k).start()

    @pl.when(inner)
    def _():
        share(1)
        x[me_s, 0] = normed[:, aligned(half, pair)]
        shares = {}
        order = [hub, edge, far_hub, 3 - edge]

        def arrival(s):
            return pltpu.make_async_remote_copy(
                src_ref=x.at[s, 0], dst_ref=x.at[s, 0], send_sem=as_.at[0], recv_sem=ar_.at[s],
                device_id={"sp": far_hub}, device_id_type=MESH,
            )

        def block(s, src, r, slot, to):
            return send(src, x.at[s, slot], bs.at[s, r], br.at[s, r], tp=to)

        for i, s in enumerate(order):
            if i:
                arrival(s).wait_recv()
            src = normed.at[:, aligned(half, pair)] if i == 0 else x.at[s, 0]
            shares[i, 1] = block(s, src, 0, 2, across)
            shares[i, 0] = block(s, src, 1, 1, mate)
        for i, s in enumerate(order):
            shares[i, 1].wait_recv()
            shares[i, 2] = block(s, x.at[s, 2], 2, 3, mate)
        share(2)
        own_loads[0].wait()
        own_loads[1].wait()
        rows = 2 * n_tp * own
        for i, s in enumerate(order):
            shares[i, 0].wait_recv()
            shares[i, 2].wait_recv()
        theirs = x[aligned(1 - half, 2)].reshape(rows, pair)
        parts = []
        for j, (a, b) in enumerate(cuts):
            if j == 1:
                share(3)
            shared(j).wait_recv()
            for k in range(2):
                part_out[k, :, a:b] = jnp.dot(
                    theirs, wgu[k, :, a:b], preferred_element_type=F32
                ).astype(BF16)
            parts.append(
                send(part_out.at[:, :, pl.ds(a, b - a)], part_in.at[:, :, pl.ds(a, b - a)],
                     cs.at[j], cr.at[j], sp=far_hub)
            )
        mine = x[aligned(half, 2)].reshape(rows, pair)
        spreads = []
        for j, (a, b) in enumerate(cuts):
            gate = jnp.dot(mine, wgu[0, :, a:b], preferred_element_type=F32)
            up = jnp.dot(mine, wgu[1, :, a:b], preferred_element_type=F32)
            parts[j].wait_recv()
            gate = gate + part_in[0, :, a:b].astype(F32)
            up = up + part_in[1, :, a:b].astype(F32)
            h[0, :, a:b] = (jax.nn.silu(gate) * up).astype(BF16)
            spreads.append(
                send(h.at[0, :, pl.ds(a, b - a)], h.at[1, :, pl.ds(a, b - a)],
                     ds.at[j], dr.at[j], sp=far_hub)
            )
            if 1 <= j <= DOWN:
                handed_down(j - 1).wait_recv()
                shared_down(j - 1).start()
        own_loads[2].wait()
        for k in range(DOWN):
            shared_down(k).wait_recv()
        slots = [0, 1, 2, 3]
        targets = [me_t, mate, across, 3 - me_t]
        sums = []
        kept = []
        for i in range(2):
            if i:
                for spread in spreads:
                    spread.wait_recv()
            y = jnp.dot(h[i], wd[...], preferred_element_type=F32).reshape(2, n_tp, own, pair)
            kept.append(y[:, 0])
            for r in (2, 3, 1):
                y_out[i, r - 1] = y[:, r].astype(BF16)
                sums.append(
                    send(y_out.at[i, r - 1], y_in.at[i, r - 1], es.at[i, r - 1], er.at[i, r - 1],
                         tp=targets[r])
                )
        backs = []
        for i in (0, 1):
            z = kept[i]
            for n in range(3):
                sums[3 * i + n].wait_recv()
            for r in range(1, n_tp):
                z = z + y_in[i, r - 1].astype(F32)
            z_out[i] = z.astype(BF16)
            if i == 0:
                at = aligned(half, pair)
                spare = me_s % 2
                out_ref[:, at] = (stream[:, at] + z_out[0, spare].astype(F32)).astype(BF16)
                copy = from_hub(edge, half, z_out.at[0, 1 - spare], None)
                copy.start()
                backs.append(copy)
            else:
                for e in range(2):
                    copy = from_hub(2 * (1 - half) + e, half, z_out.at[1, e], None)
                    copy.start()
                    backs.append(copy)
        for copy in list(shares.values()) + parts + spreads + sums + backs:
            copy.wait_send()
        for j in range(CHUNKS):
            shared(j).wait_send()
        for k in range(DOWN):
            shared_down(k).wait_send()

    for q in range(2):
        @pl.when(me_s != q + 1)
        def _():
            pltpu.make_async_remote_copy(
                src_ref=z_in.at[q], dst_ref=z_in.at[q], send_sem=gs.at[0], recv_sem=gr.at[q],
                device_id={"sp": q + 1}, device_id_type=MESH,
            ).wait_recv()
            at = pl.ds(q * pair, pair)
            out_ref[:, at] = (stream[:, at] + z_in[q].astype(F32)).astype(BF16)
            to_hub(q).wait_send()

    @pl.when(jnp.logical_not(inner))
    def _():
        for k in range(DOWN):
            handed_down(k).wait_send()


def moved_rows(
    ssm_input, residual_in, log_step, decay_real, freq, in_real, in_imag, out_real, out_imag,
    skip, w_glu, b_glu, w_branch, norm_gain, w_gate, w_up, w_down,
):
    sizes = {axis: lax.axis_size(axis) for axis in ("grp", "sp", "tp")}
    n_sp, n_tp = sizes["sp"], sizes["tp"]
    tok, width = ssm_input.shape
    groups, states = decay_real.shape
    group = in_real.shape[2]
    lanes = groups * states
    own = tok // n_tp
    chan, d_model = w_branch.shape
    depth, hid = w_gate.shape
    cols = w_down.shape[1]
    pair = 2 * depth
    vm = pl.BlockSpec(memory_space=pltpu.VMEM)
    hbm = pl.BlockSpec(memory_space=pl.ANY)
    dma = pltpu.SemaphoreType.DMA
    vmem = pltpu.VMEM
    return pl.pallas_call(
        functools.partial(layer_kernel, sizes),
        out_shape=jax.ShapeDtypeStruct((own, d_model), BF16),
        in_specs=[vm, hbm] + [vm] * 8 + [hbm, vm, hbm, vm] + [hbm] * 3,
        out_specs=vm,
        scratch_shapes=[
            vmem((own, d_model), BF16),
            vmem((own, d_model), F32),
            vmem((2, pair, hid), BF16),
            vmem((hid, 2 * cols), BF16),
            vmem((n_sp, n_tp, own, pair), BF16),
            vmem((2, 2 * tok, hid), BF16),
            vmem((2, 2 * tok, hid), BF16),
            vmem((2, 2 * tok, hid), BF16),
            vmem((2, n_tp - 1, 2, own, pair), BF16),
            vmem((2, n_tp - 1, 2, own, pair), BF16),
            vmem((2, 2, own, pair), BF16),
            vmem((2, own, pair), BF16),
            dma((3,)),
            dma((CHUNKS, 2)), dma((CHUNKS, 2)),
            dma((CHUNKS,)), dma((CHUNKS,)),
            dma((DOWN,)), dma((DOWN,)), dma((DOWN,)), dma((DOWN,)),
            dma((2,)), dma((n_sp,)),
            dma((n_sp, 3)), dma((n_sp, 3)),
            dma((CHUNKS,)), dma((CHUNKS,)), dma((CHUNKS,)), dma((CHUNKS,)),
            dma((2, n_tp - 1)), dma((2, n_tp - 1)),
            dma((n_sp,)), dma((2,)),
            vmem((chan, chan), BF16),
            vmem((chan, d_model), BF16),
            vmem((own, d_model), BF16),
            vmem((8, lanes), F32),
            vmem((tok, lanes), F32),
            vmem((tok, lanes), F32),
            vmem((tok, lanes), F32),
            vmem((tok, lanes), F32),
            vmem((2, lanes), F32),
            vmem((n_sp - 1, 2, lanes), F32),
            vmem((n_tp, own, width), BF16),
            vmem((n_tp - 1, own, width), BF16),
            vmem((own, chan), F32),
            dma((3,)),
            dma((n_sp - 1,)), dma((n_sp - 1,)),
            dma((n_tp - 1,)), dma((n_tp - 1,)),
        ],
        compiler_params=pltpu.CompilerParams(collective_id=0, has_side_effects=True),
        name="layer",
    )(
        ssm_input, residual_in, log_step[None], decay_real, freq,
        in_real.swapaxes(1, 2).reshape(width, states),
        in_imag.swapaxes(1, 2).reshape(width, states),
        out_real.reshape(width, states), out_imag.reshape(width, states),
        skip[None], w_glu, b_glu[None], w_branch, norm_gain[None], w_gate, w_up, w_down,
    )


def per_device(*arguments):
    sizes = tuple(lax.axis_size(axis) for axis in ("grp", "sp", "tp"))
    return (moved_rows if sizes == (2, 4, 4) else gathered_weights)(*arguments)


def solution(mesh):
    placed = (
        P(("grp", "sp"), "tp"),
        P(("grp", "sp"), None),
        P("tp"),
        P("tp", None),
        P("tp", None),
        P("tp", None, None),
        P("tp", None, None),
        P("tp", None, None),
        P("tp", None, None),
        P("tp"),
        P(),
        P(),
        P(),
        P(),
        P("sp", "tp"),
        P("sp", "tp"),
        P("tp", "sp"),
    )
    return jax.shard_map(
        per_device,
        mesh=mesh,
        in_specs=placed,
        out_specs=P(("grp", "sp", "tp"), None),
        check_vma=False,
    )
```
